256 devices in a mesh: sp: 32 (over z, y), tp: 8 (over x, core).
Axes of the slice: x: 4, y: 4, z: 8, core: 2. Of those that a mesh axis runs over, the one named last changes fastest.
Arguments:
- residual: bfloat16 [32768, 2048], P(('sp', 'tp')), may hold values from -6 to 6
- first_group_queries: bfloat16 [32768, 1024], P('sp', 'tp'), may hold values from -6 to 6
- first_group_keys: bfloat16 [32768, 1024], P('sp', 'tp'), may hold values from -6 to 6
- second_group_queries: bfloat16 [32768, 512], P('sp', 'tp'), may hold values from -6 to 6
- second_group_keys: bfloat16 [32768, 512], P('sp', 'tp'), may hold values from -6 to 6
- primary_retain_switch_inputs: bfloat16 [32768, 1024], P('sp', 'tp'), may hold values from -12 to 16
- secondary_retain_switch_inputs: bfloat16 [32768, 512], P('sp', 'tp'), may hold values from -12 to 16
- timestep_fading_exponent: float32 [32768], P('sp'), may hold values from -2.1 to 0
- values: bfloat16 [2, 32768, 1024], P(None, 'sp', 'tp'), may hold values from -6 to 6
- output_gate_logits: bfloat16 [2, 32768, 1024], P(None, 'sp', 'tp'), may hold values from -6 to 6
- head_norm_gains: float32 [2, 1024], P(None, 'tp'), may hold values from 0.1 to 1.9
- output_projection: bfloat16 [2, 1024, 2048], P(None, 'tp'), may hold values from -0.125 to 0.125
- feedforward_norm_gain: float32 [2048], replicated, may hold values from 0.1 to 1.9
- gate_projection: bfloat16 [2048, 6144], P('sp', 'tp'), may hold values from -0.125 to 0.125
- up_projection: bfloat16 [2048, 6144], P('sp', 'tp'), may hold values from -0.125 to 0.125
- down_projection: bfloat16 [6144, 2048], P('tp', 'sp'), may hold values from -0.078125 to 0.078125
Outputs:
- layer_out: bfloat16 [32768, 2048], P(('sp', 'tp'))
The draws below stay inside these ranges and needn't reach their ends.
All inputs are finite; a program needn't handle non-finite values.
Results may differ from the reference program's by a relative error of at most 0.018.
Values may be sent and summed in bfloat16 or wider, within the bound.
A program may use at most 128 MiB of HBM per device.

```python
import jax
import jax.numpy as jnp
from jax import lax

D = 2048
HEADS = 8
FIRST_KEY_SIZE = 128
SECOND_KEY_SIZE = 64
DV = 128
FF = 6144
BLOCK = 64
SEQ = 32768
N_TP = 8


def forget_draw(base_key, key_width):
    key_rank, key_factor, key_channel, key_jitter, key_long, key_level = jax.random.split(base_key, 6)
    ranking = jax.random.permutation(key_rank, HEADS)
    fast_count = HEADS // 2
    long_share = 0.5
    fast_mask = jnp.repeat((ranking < fast_count).astype(jnp.float32), key_width)
    slow_level = jnp.log(SEQ / 3.2)
    fast_level = -jnp.log(jnp.exp(16.0 / (0.6 * BLOCK)) - 1.0)
    long_mask = (jax.random.uniform(key_long, (HEADS * key_width,), jnp.float32) < long_share).astype(jnp.float32)
    spread_level = jax.random.uniform(key_level, (HEADS * key_width,), jnp.float32, jnp.log(4.0), slow_level)
    slow_channel = long_mask * slow_level + (1.0 - long_mask) * spread_level
    base_level = fast_mask * fast_level + (1.0 - fast_mask) * slow_channel
    factor = jax.random.uniform(key_factor, (SEQ // BLOCK, 1), jnp.float32, 0.0, jnp.log(4.0))
    factor = jnp.repeat(factor, BLOCK, axis=0)
    channel = jnp.clip(0.5 * jax.random.normal(key_channel, (1, HEADS * key_width), jnp.float32), -1.5, 1.5)
    jitter = jnp.clip(0.8 * jax.random.normal(key_jitter, (SEQ, HEADS * key_width), jnp.float32), -3.2, 3.2)
    result = base_level[None, :] - factor + channel + jitter
    return result.astype(jnp.bfloat16)


def draw_primary_retain_switch_inputs(key, part):
    return forget_draw(jax.random.fold_in(key, 11), FIRST_KEY_SIZE)


def draw_secondary_retain_switch_inputs(key, part):
    return forget_draw(jax.random.fold_in(key, 23), SECOND_KEY_SIZE)


def draw_timestep_fading_exponent(key, part):
    key_spot, key_loss = jax.random.split(jax.random.fold_in(key, 37))
    positions = jax.random.randint(key_spot, (3,), 0, SEQ)
    losses = jax.random.uniform(key_loss, (3,), jnp.float32, jnp.log(0.5), jnp.log(0.8))
    hits = jnp.arange(SEQ)[:, None] == positions[None, :]
    return jnp.sum(jnp.where(hits, losses[None, :], 0.0), axis=1).astype(jnp.float32)


def block_scale(stream_key, dims, shards, smallest, top_value):
    factor_of = 1.0
    for dim, shards_of in shards:
        draws = jax.random.uniform(jax.random.fold_in(jax.random.fold_in(stream_key, 6), dim), (shards_of,), jnp.float32, smallest / len(shards), top_value / len(shards))
        factor_of = factor_of * jnp.repeat(jnp.exp(draws), dims[dim] // shards_of).reshape((-1,) + (1,) * (len(dims) - 1 - dim))
    return factor_of


def scatter_about(key, shape, scale, limit, pieces=(), kind=jnp.bfloat16):
    entries = scale * jax.random.normal(key, shape, jnp.float32)
    if pieces:
        entries = entries * block_scale(key, shape, pieces, -0.22, 0.18)
    return jnp.clip(entries, -limit, limit).astype(kind)


def setup_inputs(seed: int = 0) -> dict:
    streams_of = jax.random.split(jax.random.key(seed), 17)
    return {
        "residual": scatter_about(streams_of[0], (SEQ, D), 1.0, 6.0, ((0, 256),)),
        "first_group_queries": scatter_about(streams_of[1], (SEQ, HEADS * FIRST_KEY_SIZE), 1.0, 6.0, ((0, 32), (1, 8))),
        "first_group_keys": scatter_about(streams_of[2], (SEQ, HEADS * FIRST_KEY_SIZE), 1.0, 6.0, ((0, 32), (1, 8))),
        "second_group_queries": scatter_about(streams_of[3], (SEQ, HEADS * SECOND_KEY_SIZE), 1.0, 6.0, ((0, 32), (1, 8))),
        "second_group_keys": scatter_about(streams_of[4], (SEQ, HEADS * SECOND_KEY_SIZE), 1.0, 6.0, ((0, 32), (1, 8))),
        "primary_retain_switch_inputs": draw_primary_retain_switch_inputs(jax.random.fold_in(streams_of[16], 71), 0),
        "secondary_retain_switch_inputs": draw_secondary_retain_switch_inputs(jax.random.fold_in(streams_of[16], 71), 0),
        "timestep_fading_exponent": draw_timestep_fading_exponent(jax.random.fold_in(streams_of[16], 71), 0),
        "values": scatter_about(streams_of[8], (2, SEQ, HEADS * DV), 1.0, 6.0, ((1, 32), (2, 8))),
        "output_gate_logits": scatter_about(streams_of[9], (2, SEQ, HEADS * DV), 1.0, 6.0, ((1, 32), (2, 8))),
        "head_norm_gains": jnp.clip(1.0 + 0.18 * jax.random.normal(streams_of[10], (2, HEADS * DV), jnp.float32), 0.1, 1.9),
        "output_projection": scatter_about(streams_of[11], (2, HEADS * DV, D), (2 * HEADS * DV) ** -0.5, 0.125, ((1, 8),)),
        "feedforward_norm_gain": jnp.clip(1.0 + 0.18 * jax.random.normal(streams_of[12], (D,), jnp.float32), 0.1, 1.9),
        "gate_projection": scatter_about(streams_of[13], (D, FF), D ** -0.5, 0.125, ((0, 32), (1, 8))),
        "up_projection": scatter_about(streams_of[14], (D, FF), D ** -0.5, 0.125, ((0, 32), (1, 8))),
        "down_projection": scatter_about(streams_of[15], (FF, D), FF ** -0.5, 0.078125, ((0, 8), (1, 32))),
    }


EPS = 1e-06
SOFTNESS_SCALE = 16.0
highest_precision = lax.Precision.HIGHEST

def blocks(source, block_count, head_count, key_width):
    return source.astype(jnp.float32).reshape(block_count, BLOCK, head_count, key_width).transpose(0, 2, 1, 3)

def mechanism(query_matrix_rows, key_matrix_rows, value_matrix_rows, decay_logarithm, key_width):
    block_count = query_matrix_rows.shape[0] // BLOCK
    query_blocks = blocks(query_matrix_rows, block_count, HEADS, key_width) * key_width ** (-0.5)
    key_blocks = blocks(key_matrix_rows, block_count, HEADS, key_width)
    value_blocks = blocks(value_matrix_rows, block_count, HEADS, DV)
    decay_blocks = jnp.cumsum(blocks(decay_logarithm, block_count, HEADS, key_width), axis=2)
    causal = jnp.tril(jnp.ones((BLOCK, BLOCK), dtype=bool))

    def advance(running_state, inputs):
        query_piece, key_piece, value_piece, decay_piece = inputs
        spread_log = decay_piece[:, :, None, :] - decay_piece[:, None, :, :]
        decay_grid = jnp.exp(jnp.where(causal[None, :, :, None], spread_log, -jnp.inf))
        scores = lax.optimization_barrier(jnp.sum(query_piece[:, :, None, :] * key_piece[:, None, :, :] * decay_grid, axis=-1))
        block_result = jnp.einsum('hij,hjv->hiv', scores, value_piece, precision=highest_precision)
        block_result = block_result + jnp.einsum('rus,rsp->rup', query_piece * jnp.exp(decay_piece), running_state, precision=highest_precision)
        final_log_decay = decay_piece[:, -1:, :]
        running_state = jnp.exp(final_log_decay[:, 0, :])[:, :, None] * running_state + jnp.einsum('qxe,qxt->qet', key_piece * jnp.exp(final_log_decay - decay_piece), value_piece, precision=highest_precision)
        return (running_state, block_result)
    zero_state = jnp.zeros((HEADS, key_width, DV), jnp.float32)
    _, outputs = lax.scan(advance, zero_state, (query_blocks, key_blocks, value_blocks, decay_blocks))
    return outputs.transpose(0, 2, 1, 3).reshape(query_matrix_rows.shape[0], HEADS, DV)

def gate_heads(head_out, gate_rows, gain_row):
    inverse = lax.rsqrt(lax.optimization_barrier(jnp.mean(head_out * head_out, axis=-1, keepdims=True)) + EPS)
    normed = (head_out * inverse).reshape(head_out.shape[0], -1) * gain_row
    return (jax.nn.silu(gate_rows.astype(jnp.float32)) * normed).astype(jnp.bfloat16)

def grouped_product(left_sides, right_sides):
    portion = left_sides[0].shape[1] // N_TP
    row_count = left_sides[0].shape[0]
    col_count = right_sides[0].shape[1]

    def add_group(group_index, summed):
        offset = (group_index * portion).astype(jnp.int32)
        partial_value = jnp.zeros((row_count, col_count), jnp.float32)
        for left_side, right_side in zip(left_sides, right_sides):
            partial_value = partial_value + jnp.dot(lax.dynamic_slice_in_dim(left_side, offset, portion, 1), lax.dynamic_slice_in_dim(right_side, offset, portion, 0), preferred_element_type=jnp.float32)
        rounded = lax.optimization_barrier(partial_value.astype(jnp.bfloat16))
        return summed + rounded.astype(jnp.float32)
    return lax.fori_loop(0, N_TP, add_group, jnp.zeros((row_count, col_count), jnp.float32))

def row_norm(source, gain_row):
    widened = source.astype(jnp.float32)
    inverse = lax.rsqrt(lax.optimization_barrier(jnp.mean(widened * widened, axis=-1, keepdims=True)) + EPS)
    return (widened * inverse * gain_row).astype(jnp.bfloat16)

def reference(residual, first_group_queries, first_group_keys, second_group_queries, second_group_keys, primary_retain_switch_inputs, secondary_retain_switch_inputs, timestep_fading_exponent, values, output_gate_logits, head_norm_gains, output_projection, feedforward_norm_gain, gate_projection, up_projection, down_projection):
    primary_fading_exponent = jax.nn.log_sigmoid(primary_retain_switch_inputs.astype(jnp.float32)) / SOFTNESS_SCALE + timestep_fading_exponent[:, None]
    secondary_fading_exponent = jax.nn.log_sigmoid(secondary_retain_switch_inputs.astype(jnp.float32)) / SOFTNESS_SCALE + timestep_fading_exponent[:, None]
    heads_a = mechanism(first_group_queries, first_group_keys, values[0], primary_fading_exponent, FIRST_KEY_SIZE)
    heads_b = mechanism(second_group_queries, second_group_keys, values[1], secondary_fading_exponent, SECOND_KEY_SIZE)
    gated_a = gate_heads(heads_a, output_gate_logits[0], head_norm_gains[0])
    gated_b = gate_heads(heads_b, output_gate_logits[1], head_norm_gains[1])
    attention = grouped_product((gated_a, gated_b), (output_projection[0], output_projection[1]))
    mid_rows = (residual.astype(jnp.float32) + attention).astype(jnp.bfloat16)
    normed = row_norm(mid_rows, feedforward_norm_gain)
    gate_sum = jnp.dot(normed, gate_projection, preferred_element_type=jnp.float32)
    up_sum = jnp.dot(normed, up_projection, preferred_element_type=jnp.float32)
    hidden = (jax.nn.silu(gate_sum) * up_sum).astype(jnp.bfloat16)
    down_sum = grouped_product((hidden,), (down_projection,))
    return (mid_rows.astype(jnp.float32) + down_sum).astype(jnp.bfloat16)
```

```python
import functools

import jax
import jax.numpy as jnp
from jax import lax
from jax.experimental import pallas as pl
from jax.experimental.pallas import tpu as pltpu
from jax.sharding import Mesh
from jax.sharding import PartitionSpec as P

SP = ("sp_0", "sp_1")
TP = ("tp_0", "tp_1")
SP_TP = ("sp_0", "sp_1", "tp_0", "tp_1")
EPS = 1e-06
MESH = pl.DeviceIdType.MESH
BF16, F32 = jnp.bfloat16, jnp.float32

NZ, NY, NX = 8, 4, 4
CH = 128
NCH = 8
KA, KB = 128, 64
FF = 768
WR = 192
XR = 80
XCUT = 48
YCUT = XR + 64
DT = (((1,), (1,)), ((), ()))
TD = (((0,), (0,)), ((), ()))


def dot(a, b):
    return jnp.dot(a, b, preferred_element_type=F32)


def dotg(a, b, dims):
    return lax.dot_general(a, b, dims, preferred_element_type=F32)


class Net:
    def __init__(self, ssem, rsem):
        self.ssem, self.rsem = ssem, rsem
        self.z, self.y = lax.axis_index("sp_0"), lax.axis_index("sp_1")
        self.x, self.c = lax.axis_index("tp_0"), lax.axis_index("tp_1")
        self.count = 0
        self.sent = []

    def number(self):
        self.count += 1
        return self.count - 1

    def at_z(self, k):
        return lax.rem(self.z + (k + NZ), NZ)

    def at_y(self, k):
        return lax.rem(self.y + (k + NY), NY)

    def at_x(self, k):
        return lax.rem(self.x + (k + NX), NX)

    def to_z(self, k):
        return (self.at_z(k), self.y, self.x, self.c)

    def to_y(self, k):
        return (self.z, self.at_y(k), self.x, self.c)

    def to_x(self, k):
        return (self.z, self.y, self.at_x(k), self.c)

    def partner(self):
        return (self.z, self.y, self.x, 1 - self.c)

    def _copy(self, src, dst, number, device):
        return pltpu.make_async_remote_copy(
            src_ref=src,
            dst_ref=dst,
            send_sem=self.ssem.at[number],
            recv_sem=self.rsem.at[number],
            device_id=device,
            device_id_type=MESH,
        )

    def send(self, src, dst, number, device):
        copy = self._copy(src, dst, number, device)
        copy.start()
        self.sent.append(copy)

    def arrived(self, dst, number):
        self._copy(dst, dst, number, self.partner()).wait_recv()

    def drain(self):
        for copy in self.sent:
            copy.wait_send()

    def greet(self):
        barrier = pltpu.get_barrier_semaphore()
        peers = [self.partner()]
        peers += [self.to_x(k) for k in (1, -1)]
        peers += [self.to_y(k) for k in range(1, NY)]
        peers += [self.to_z(k) for k in range(1, NZ)]
        for device in peers:
            pl.semaphore_signal(barrier, inc=1, device_id=device, device_id_type=MESH)
        pl.semaphore_wait(barrier, len(peers))


class Weights:
    def __init__(self, net, w, wg, lsem):
        self.net, self.w, self.wg, self.lsem = net, w, wg, lsem
        n = net.number
        self.xb = [n(), n()]
        self.xf = [n(), n()]
        self.xz = [[n(), n()] for _ in range(NZ // 2)]
        self.yz = [[n(), n()] for _ in range(NZ // 2)]
        self.yb = [[n(), n()] for _ in range(NZ)]
        self.yf = [[n(), n()] for _ in range(NZ)]

    def own(self):
        net = self.net
        self.local = pltpu.make_async_copy(self.w, self.wg.at[net.z, net.y], self.lsem)
        self.local.start()

    def own_done(self):
        self.local.wait()

    def x_slot(self, ky, lo, hi):
        return self.wg.at[self.net.z, self.net.at_y(ky), lo:hi]

    def x_out(self):
        net = self.net
        for d, k in enumerate((1, -1)):
            net.send(self.w.at[0:XR], self.x_slot(0, 0, XR), self.xb[d], net.to_y(k))

    def x_forward(self):
        net = self.net
        for d, (k, lo, hi) in enumerate(((1, 0, XCUT), (-1, XCUT, XR))):
            net.arrived(self.x_slot(-k, 0, XR), self.xb[d])
            part = self.x_slot(-k, lo, hi)
            net.send(part, part, self.xf[d], net.to_y(k))

    def x_forwarded(self):
        for d, (lo, hi) in enumerate(((0, XCUT), (XCUT, XR))):
            self.net.arrived(self.x_slot(2, lo, hi), self.xf[d])

    def x_bundle(self, kz, s, d):
        lo, hi = (0, NY) if s < NZ // 2 else ((0, NY // 2) if d == 0 else (NY // 2, NY))
        return self.wg.at[self.net.at_z(kz), lo:hi, 0:XR]

    def xz_send(self, s):
        for d, k in enumerate((1, -1)):
            part = self.x_bundle(-k * (s - 1), s, d)
            self.net.send(part, part, self.xz[s - 1][d], self.net.to_z(k))

    def xz_wait(self, s):
        for d, k in enumerate((1, -1)):
            self.net.arrived(self.x_bundle(-k * s, s, d), self.xz[s - 1][d])

    def y_rows(self, s, d):
        return (XR, WR) if s < NZ // 2 else ((XR, YCUT) if d == 0 else (YCUT, WR))

    def y_slot(self, kz, lo, hi, ky=0):
        return self.wg.at[self.net.at_z(kz), self.net.at_y(ky), lo:hi]

    def yz_send(self, s):
        net = self.net
        for d, k in enumerate((1, -1)):
            lo, hi = self.y_rows(s, d)
            part = self.y_slot(-k * (s - 1), lo, hi)
            src = self.w.at[lo:hi] if s == 1 else part
            net.send(src, part, self.yz[s - 1][d], net.to_z(k))

    def yz_wait(self, s):
        for d, k in enumerate((1, -1)):
            lo, hi = self.y_rows(s, d)
            self.net.arrived(self.y_slot(-k * s, lo, hi), self.yz[s - 1][d])

    def yb_send(self, kz):
        net = self.net
        slot = self.y_slot(kz, XR, WR)
        src = self.w.at[XR:WR] if kz == 0 else slot
        for d, k in enumerate((1, -1)):
            net.send(src, slot, self.yb[kz % NZ][d], net.to_y(k))

    def yf_send(self, kz):
        net = self.net
        for d, (k, lo, hi) in enumerate(((1, XR, YCUT), (-1, YCUT, WR))):
            net.arrived(self.y_slot(kz, XR, WR, -k), self.yb[kz % NZ][d])
            part = self.y_slot(kz, lo, hi, -k)
            net.send(part, part, self.yf[kz % NZ][d], net.to_y(k))

    def yf_wait(self, kz):
        for d, (lo, hi) in enumerate(((XR, YCUT), (YCUT, WR))):
            self.net.arrived(self.y_slot(kz, lo, hi, 2), self.yf[kz % NZ][d])


def rows_of(chunk, size=CH):
    return pl.ds(pl.multiple_of(chunk * size, size), size)


def iotas(n):
    return (
        lax.broadcasted_iota(jnp.int32, (n, n), 0),
        lax.broadcasted_iota(jnp.int32, (n, n), 1),
    )


class Attention:
    def __init__(self, net, r):
        self.net, self.r = net, r
        n = net.number
        self.m1 = [n() for _ in range(NY)]
        self.m2 = [n() for _ in range(NZ)]
        self.m3 = [n() for _ in range(NY)]
        self.heads = (
            (KA, r["qa"], r["ka"], r["ga"], r["ba"], r["sa"], r["ea"], r["pa"], r["ta"], 0),
            (KB, r["qb"], r["kb"], r["gb"], r["bb"], r["sb"], r["eb"], r["pb"], r["tb"], 1),
        )

    def states(self):
        r = self.r
        row, col = iotas(CH)
        lower = row >= col
        tri = jnp.where(lower, 1.0, 0.0).astype(BF16)
        tri2 = jnp.concatenate([tri, tri], axis=1)

        def step(c, carry):
            rows = rows_of(c)
            line = r["fade"][pl.ds(c, 1), :]
            fade = jnp.sum(jnp.where(lower, line, 0.0), axis=1, keepdims=True)
            new = []
            for (width, q, k, g, b, s, e, p, t, h), (state, before) in zip(self.heads, carry):
                x = g[rows, :].astype(F32)
                slow = (jnp.minimum(x, 0.0) - jnp.log1p(jnp.exp(-jnp.abs(x)))) * (1.0 / 16.0)
                high = slow.astype(BF16)
                low = (slow - high.astype(F32)).astype(BF16)
                sums = dot(tri2, jnp.concatenate([high, low], axis=0)) + fade
                b[rows, :] = sums
                total = sums[CH - 1 : CH, :]
                faded = (k[rows, :].astype(F32) * jnp.exp(total - sums)).astype(BF16)
                s[c] = state
                e[pl.ds(c, 1), :] = before
                state = jnp.exp(total) * state + dotg(r["v"][h, rows, :], faded, TD)
                new.append((state, before + total))
            return tuple(new)

        zero = tuple(
            (jnp.zeros((CH, width), F32), jnp.zeros((1, width), F32)) for width in (KA, KB)
        )
        (state_a, log_a), (state_b, log_b) = lax.fori_loop(0, NCH, step, zero)
        out = r["m1s"]
        quarter = CH // NY
        row16 = lax.broadcasted_iota(jnp.int32, (16, 1), 0)

        def two_rows(value):
            high = value.astype(BF16).astype(F32)
            return jnp.where(row16 == 0, high, value - high).astype(BF16)

        ends_a, ends_b = two_rows(jnp.exp(log_a)), two_rows(jnp.exp(log_b))
        for i in range(NY):
            part = slice(i * quarter, (i + 1) * quarter)
            out[i, 0:quarter, 0:KA] = state_a[part].astype(BF16)
            out[i, 0:quarter, KA : KA + KB] = state_b[part].astype(BF16)
            out[i, 0:quarter, KA + KB :] = jnp.zeros((quarter, KB), BF16)
            out[i, quarter:, 0:KA] = ends_a
            out[i, quarter:, KA : KA + KB] = ends_b
            out[i, quarter:, KA + KB :] = jnp.zeros((16, KB), BF16)

    def send_quarters(self):
        net, r = self.net, self.r
        for k in range(1, NY):
            net.send(r["m1s"].at[net.at_y(k)], r["m1r"].at[k], self.m1[k], net.to_y(k))

    @staticmethod
    def opened(message):
        quarter = CH // NY
        state = message[0:quarter, :].astype(F32)
        decay = message[quarter : quarter + 1, :].astype(F32) + message[
            quarter + 1 : quarter + 2, :
        ].astype(F32)
        return state, decay

    def send_line_total(self):
        net, r = self.net, self.r
        quarter = CH // NY
        for k in range(1, NY):
            net.arrived(r["m1r"].at[k], self.m1[k])
        r["m1r"][0] = r["m1s"][net.y]
        state = jnp.zeros((quarter, 256), F32)
        decay = jnp.ones((1, 256), F32)
        for i in range(NY):
            slot = lax.rem(net.y - i + NY, NY)
            own, factor = self.opened(r["m1r"][slot])
            state, decay = factor * state + own, factor * decay
        row16 = lax.broadcasted_iota(jnp.int32, (16, 1), 0)
        high = decay.astype(BF16).astype(F32)
        r["m2s"][0:quarter, :] = state.astype(BF16)
        r["m2s"][quarter:, :] = jnp.where(row16 == 0, high, decay - high).astype(BF16)
        for k in (1, -1, 2, -2, 3, -3, 4):
            net.send(r["m2s"], r["m2r"].at[k % NZ], self.m2[k % NZ], net.to_z(k))

    def send_incoming(self):
        net, r = self.net, self.r
        quarter = CH // NY
        for k in range(1, NZ):
            net.arrived(r["m2r"].at[k], self.m2[k])
        r["m2r"][0] = jnp.zeros((48, 256), BF16)
        state = jnp.zeros((quarter, 256), F32)
        for i in range(NZ - 1):
            slot = lax.rem(net.z - i + NZ, NZ)
            own, factor = self.opened(r["m2r"][slot])
            state = jnp.where(i < net.z, factor * state + own, state)
        for i in range(NY):
            r["m3s"][i] = state.astype(BF16)
            slot = lax.rem(net.y - i + NY, NY)
            own, factor = self.opened(r["m1r"][slot])
            state = factor * state + own
        for k in range(1, NY):
            net.send(r["m3s"].at[net.at_y(k)], r["m3r"].at[net.y], self.m3[k], net.to_y(k))
        r["m3r"][net.y] = r["m3s"][net.y]

    def incoming(self):
        net, r = self.net, self.r
        for k in range(1, NY):
            net.arrived(r["m3r"].at[net.at_y(-k)], self.m3[k])

    def scores(self, start, stop):
        r = self.r
        row, col = iotas(CH)
        near = ((row >> 5) == (col >> 5)) & (row >= col)
        middle = ((row >> 6) == (col >> 6)) & ((row >> 5) > (col >> 5))
        far = (row >> 6) > (col >> 6)

        def around(sums, size, at):
            width = sums.shape[1]
            parts = sums.reshape(CH // size, size, width)
            return (parts - parts[:, at : at + 1, :]).reshape(CH, width)

        def step(c, carry):
            rows = rows_of(c)
            for width, q, k, g, b, s, e, p, t, h in self.heads:
                sums = b[rows, :]
                query = q[rows, :].astype(F32) * (width**-0.5)
                key = k[rows, :].astype(F32)
                t[rows, :] = (query * jnp.exp(sums)).astype(BF16)
                at = around(sums, 32, 15)
                local = dotg(
                    (query * jnp.exp(at)).astype(BF16), (key * jnp.exp(-at)).astype(BF16), DT
                )
                total = jnp.where(near, local, 0.0)
                for size, at, mask in ((64, 31, middle), (128, 63, far)):
                    f = jnp.exp(-jnp.abs(around(sums, size, at)))
                    wide = dotg((query * f).astype(BF16), (key * f).astype(BF16), DT)
                    total = jnp.where(mask, wide, total)
                p[c] = total.astype(BF16)
            return carry

        lax.fori_loop(start, stop, step, 0)

    def gated(self, first, count):
        r = self.r

        def step(i, carry):
            c = first + i
            rows = rows_of(c)
            before_state = r["m3r"][...].astype(F32).reshape(CH, 256)
            for width, q, k, g, b, s, e, p, t, h in self.heads:
                state = s[c] + jnp.exp(e[pl.ds(c, 1), :]) * before_state[:, h * KA : h * KA + width]
                out = dot(p[c], r["v"][h, rows, :]) + dotg(t[rows, :], state.astype(BF16), DT)
                inverse = lax.rsqrt(jnp.mean(out * out, axis=-1, keepdims=True) + EPS)
                gate = r["og"][h, rows, :].astype(F32)
                normed = out * inverse * r["gain"][h : h + 1, :]
                value = gate * jax.nn.sigmoid(gate) * normed
                r["gat"][rows, h * CH : (h + 1) * CH] = value.astype(BF16)
            return carry

        lax.fori_loop(0, count, step, 0)


HALF = 1024
BLK = 256
LEFT, RIGHT = slice(0, 512), slice(512, 1024)


class Reduce:
    def __init__(self, net, part, comb, hop, joined, direct):
        self.net, self.part, self.comb = net, part, comb
        self.hop, self.joined, self.direct = hop, joined, direct
        n = net.number
        self.h = [[n(), n()] for _ in range(2)]
        self.j = [[n(), n()] for _ in range(2)]
        self.d = [n(), n()]

    def send_far(self):
        net = self.net
        for piece in range(2):
            rows = pl.ds(piece * CH, CH)
            for side, (k, cols) in enumerate(((1, LEFT), (-1, RIGHT))):
                net.send(
                    self.part.at[0, rows, cols],
                    self.hop.at[side, rows],
                    self.h[side][piece],
                    net.to_x(k),
                )

    def send_near(self):
        net = self.net
        for side, (k, block, cols) in enumerate(((1, 1, RIGHT), (-1, 2, LEFT))):
            net.send(
                self.part.at[block, :, cols], self.direct.at[side], self.d[side], net.to_x(k)
            )

    def join(self):
        net = self.net
        for piece in range(2):
            rows = slice(piece * CH, (piece + 1) * CH)
            for side, (k, block, cols) in enumerate(((1, 1, LEFT), (-1, 2, RIGHT))):
                net.arrived(self.hop.at[side, rows], self.h[side][piece])
                both = self.part[block, rows, cols].astype(F32) + self.hop[side, rows, :].astype(
                    F32
                )
                self.comb[side, rows, :] = both.astype(BF16)
                net.send(
                    self.comb.at[side, rows],
                    self.joined.at[side, rows],
                    self.j[side][piece],
                    net.to_x(k),
                )

    def arrived(self, piece):
        net = self.net
        rows = slice(piece * CH, (piece + 1) * CH)
        if piece == 0:
            for side in range(2):
                net.arrived(self.direct.at[side], self.d[side])
        for side in range(2):
            net.arrived(self.joined.at[side, rows], self.j[side][piece])

    def total(self, own, rows):
        left = (
            own[rows, LEFT]
            + self.joined[0, rows, :].astype(F32)
            + self.direct[1, rows, :].astype(F32)
        )
        right = (
            own[rows, RIGHT]
            + self.joined[1, rows, :].astype(F32)
            + self.direct[0, rows, :].astype(F32)
        )
        return left, right


class Feed:
    def __init__(self, net, r):
        self.net, self.r = net, r
        n = net.number
        self.n_res, self.n_wo, self.n_ss, self.n_out, self.n_dp = n(), n(), n(), n(), n()
        self.n_gat = [n() for _ in range(NX)]
        self.n_hid = [n() for _ in range(NX)]
        self.ring = [[n(), n()] for _ in range(2)]
        self.far = [n(), n()]
        self.over = [[n(), n()] for _ in range(NX)]
        self.first = Reduce(net, r["p1"], r["c1"], r["h1"], r["j1"], r["d1"])
        self.second = Reduce(net, r["p2"], r["c2"], r["h2"], r["j2"], r["d2"])

    def cols(self, core):
        return pl.ds(pl.multiple_of(core * HALF, HALF), HALF)

    def block(self, k):
        return rows_of(self.net.at_x(k), BLK)

    def swap_inputs(self):
        net, r = self.net, self.r
        other = 1 - net.c
        net.send(
            r["res"].at[:, self.cols(other)], r["resp"], self.n_res, net.partner()
        )
        net.send(r["wo"].at[:, :, self.cols(other)], r["wop"], self.n_wo, net.partner())

    def send_gated(self, k):
        net, r = self.net, self.r
        rows = self.block(k)
        net.send(r["gat"].at[rows], r["gatp"].at[rows], self.n_gat[k % NX], net.partner())

    def swapped_projection(self):
        self.net.arrived(self.r["wop"], self.n_wo)

    def project(self, k):
        net, r = self.net, self.r
        rows = self.block(k)
        net.arrived(r["gatp"].at[rows], self.n_gat[k % NX])
        mine, theirs = r["gat"][rows, :], r["gatp"][rows, :]
        for side in range(2):
            cols = slice(side * 512, (side + 1) * 512)
            at = pl.ds(pl.multiple_of(net.c * HALF + side * 512, 512), 512)
            part = dot(mine, r["wo"][:, :, at].reshape(2 * CH, 512)) + dot(
                theirs, r["wop"][:, :, cols].reshape(2 * CH, 512)
            )
            if k == 0:
                r["own1"][:, cols] = part
            else:
                r["p1"][{2: 0, 1: 1, -1: 2}[k], :, cols] = part.astype(BF16)

    def middle(self):
        net, r = self.net, self.r
        net.arrived(r["resp"], self.n_res)
        for piece in range(2):
            self.first.arrived(piece)
            rows = slice(piece * CH, (piece + 1) * CH)
            left, right = self.first.total(r["own1"], rows)
            mine = r["res"][:, self.cols(net.c)]
            theirs = r["resp"][...]
            base = jnp.where(net.c == piece, mine.astype(F32), theirs.astype(F32))
            mid_l = (base[:, LEFT] + left).astype(BF16)
            mid_r = (base[:, RIGHT] + right).astype(BF16)
            r["mid"][rows, LEFT] = mid_l
            r["mid"][rows, RIGHT] = mid_r
            mid_l, mid_r = mid_l.astype(F32), mid_r.astype(F32)
            squares = jnp.sum(mid_l * mid_l, axis=-1, keepdims=True) + jnp.sum(
                mid_r * mid_r, axis=-1, keepdims=True
            )
            r["ss"][rows, :] = jnp.broadcast_to(squares, (CH, 128))
        net.send(r["ss"], r["ssp"], self.n_ss, net.partner())
        net.arrived(r["ssp"], self.n_ss)
        inverse = lax.rsqrt((r["ss"][...] + r["ssp"][...])[:, 0:1] * (1.0 / 2048.0) + EPS)
        gain = r["fgain"][:, self.cols(net.c)]
        normed = (r["mid"][...].astype(F32) * inverse * gain).astype(BF16)
        r["all"][net.c, self.block(0), :] = normed

    def piece(self, k, half):
        start = self.net.at_x(k) * BLK + half * CH
        return self.r["all"].at[self.net.c, pl.ds(pl.multiple_of(start, CH), CH)]

    def over_send(self, k, half):
        part = self.piece(k, half)
        self.net.send(part, part, self.over[k % NX][half], self.net.partner())

    def over_wait(self, k):
        for half in range(2):
            start = self.net.at_x(k) * BLK + half * CH
            dst = self.r["all"].at[1 - self.net.c, pl.ds(pl.multiple_of(start, CH), CH)]
            self.net.arrived(dst, self.over[k % NX][half])

    def rows_out(self):
        net = self.net
        for order in range(2):
            for d, k in enumerate((1, -1)):
                half = order if d == 0 else 1 - order
                part = self.piece(0, half)
                net.send(part, part, self.ring[d][half], net.to_x(k))
            self.over_send(0, order)

    def rows_on(self):
        net = self.net
        for d, (k, half) in enumerate(((1, 0), (-1, 1))):
            part = self.piece(-k, half)
            net.arrived(part, self.ring[d][half])
            net.send(part, part, self.far[d], net.to_x(k))
            self.over_send(-k, half)

    def rows_rest(self):
        net = self.net
        for d, (k, half) in enumerate(((1, 1), (-1, 0))):
            net.arrived(self.piece(-k, half), self.ring[d][half])
            self.over_send(-k, half)

    def rows_far(self):
        for d, half in enumerate((0, 1)):
            self.net.arrived(self.piece(2, half), self.far[d])
            self.over_send(2, half)

    def hidden(self, k):
        net, r = self.net, self.r
        rows = self.block(k)

        def step(n, carry):
            at = pl.ds(pl.multiple_of(n * 256, 256), 256)
            sums = []
            for low in (0, 128):
                total = None
                for half in range(2):
                    w = r["wg"][half * 4 : half * 4 + 4, :, low : low + 64, at]
                    part = dot(r["all"][half, rows, :], w.reshape(HALF, 256))
                    total = part if total is None else total + part
                sums.append(total)
            gate, up = sums
            r["hid"][rows, at] = (gate * jax.nn.sigmoid(gate) * up).astype(BF16)
            return carry

        lax.fori_loop(0, FF // 256, step, 0)
        net.send(r["hid"].at[rows], r["hidp"].at[rows], self.n_hid[k % NX], net.partner())

    def swap_down(self):
        net, r = self.net, self.r
        part = r["wg"].at[pl.ds(4 * (1 - net.c), 4), :, 64:128, :]
        net.send(part, r["dp"], self.n_dp, net.partner())

    def swapped_down(self):
        self.net.arrived(self.r["dp"], self.n_dp)

    def down(self, k):
        net, r = self.net, self.r
        rows = self.block(k)
        net.arrived(r["hidp"].at[rows], self.n_hid[k % NX])

        def step(n, carry):
            at = pl.ds(pl.multiple_of(n * 256, 256), 256)
            w = r["wg"][4 * net.c + n, :, 64:128, :].reshape(256, FF)
            part = dotg(r["hid"][rows, :], w, DT) + dotg(
                r["hidp"][rows, :], r["dp"][n].reshape(256, FF), DT
            )
            if k == 0:
                r["own2"][:, at] = part
            else:
                r["p2"][{2: 0, 1: 1, -1: 2}[k], :, at] = part.astype(BF16)
            return carry

        lax.fori_loop(0, HALF // 256, step, 0)

    def finish(self):
        net, r = self.net, self.r
        for piece in range(2):
            self.second.arrived(piece)
            rows = slice(piece * CH, (piece + 1) * CH)
            left, right = self.second.total(r["own2"], rows)
            r["outs"][piece, :, LEFT] = (r["mid"][rows, LEFT].astype(F32) + left).astype(BF16)
            r["outs"][piece, :, RIGHT] = (r["mid"][rows, RIGHT].astype(F32) + right).astype(BF16)
        net.send(r["outs"].at[1 - net.c], r["outp"], self.n_out, net.partner())
        r["out"][:, self.cols(net.c)] = r["outs"][net.c]
        net.arrived(r["outp"], self.n_out)
        r["out"][:, self.cols(1 - net.c)] = r["outp"][...]


INPUTS = ["res", "qa", "ka", "qb", "kb", "ga", "gb", "fade", "v", "og", "gain", "wo", "fgain", "w"]
SCRATCH = dict(
    wg=((NZ, NY, WR, FF), BF16),
    ba=((1024, KA), F32),
    bb=((1024, KB), F32),
    sa=((NCH, CH, KA), F32),
    sb=((NCH, CH, KB), F32),
    ea=((NCH, KA), F32),
    eb=((NCH, KB), F32),
    pa=((NCH, CH, CH), BF16),
    pb=((NCH, CH, CH), BF16),
    ta=((1024, KA), BF16),
    tb=((1024, KB), BF16),
    m1s=((NY, 48, 256), BF16),
    m1r=((NY, 48, 256), BF16),
    m2s=((48, 256), BF16),
    m2r=((NZ, 48, 256), BF16),
    m3s=((NY, 32, 256), BF16),
    m3r=((NY, 32, 256), BF16),
    gat=((1024, 256), BF16),
    gatp=((1024, 256), BF16),
    wop=((2, CH, HALF), BF16),
    resp=((CH, HALF), BF16),
    own1=((BLK, HALF), F32),
    p1=((3, BLK, HALF), BF16),
    c1=((2, BLK, 512), BF16),
    h1=((2, BLK, 512), BF16),
    j1=((2, BLK, 512), BF16),
    d1=((2, BLK, 512), BF16),
    mid=((BLK, HALF), BF16),
    ss=((BLK, 128), F32),
    ssp=((BLK, 128), F32),
    all=((2, 1024, HALF), BF16),
    hid=((1024, FF), BF16),
    hidp=((1024, FF), BF16),
    dp=((4, NY, 64, FF), BF16),
    own2=((BLK, HALF), F32),
    p2=((3, BLK, HALF), BF16),
    c2=((2, BLK, 512), BF16),
    h2=((2, BLK, 512), BF16),
    j2=((2, BLK, 512), BF16),
    d2=((2, BLK, 512), BF16),
    outs=((2, CH, HALF), BF16),
    outp=((CH, HALF), BF16),
)
COPIES = 128


def kernel(*refs):
    names = INPUTS + ["out"] + list(SCRATCH)
    r = dict(zip(names, refs))
    lsem, ssem, rsem = refs[len(names) :]
    net = Net(ssem, rsem)
    weights = Weights(net, r["w"], r["wg"], lsem)
    attention = Attention(net, r)
    feed = Feed(net, r)
    assert net.count <= COPIES, net.count
    net.greet()
    weights.own()
    weights.x_out()
    weights.yz_send(1)
    feed.swap_inputs()
    attention.states()
    attention.send_quarters()
    weights.x_forward()
    weights.yz_wait(1)
    weights.yz_send(2)
    weights.yb_send(0)
    attention.scores(0, 3)
    attention.send_line_total()
    attention.scores(3, 8)
    weights.own_done()
    weights.yz_wait(2)
    weights.yz_send(3)
    attention.send_incoming()
    weights.x_forwarded()
    weights.xz_send(1)
    for k in (1, -1, 2, -2):
        weights.yb_send(k)
    weights.yz_wait(3)
    weights.yz_send(4)
    attention.incoming()
    feed.swapped_projection()
    for k in (2, 1, -1, 0):
        attention.gated(2 * net.at_x(k), 2)
        feed.send_gated(k)
        if k == 1:
            feed.project(2)
            feed.first.send_far()
    feed.project(1)
    feed.project(-1)
    feed.first.send_near()
    feed.project(0)
    weights.yf_send(0)
    weights.yz_wait(4)
    for k in (3, -3, 4):
        weights.yb_send(k)
    weights.xz_wait(1)
    weights.xz_send(2)
    feed.first.join()
    weights.yf_send(1)
    weights.yf_send(-1)
    weights.xz_wait(2)
    weights.xz_send(3)
    feed.middle()
    feed.rows_out()
    weights.yf_send(2)
    weights.yf_send(-2)
    weights.xz_wait(3)
    weights.xz_send(4)
    feed.rows_on()
    weights.yf_send(3)
    weights.yf_send(-3)
    weights.yf_send(4)
    for k in (0, 1, -1, 2, -2, 3, -3, 4):
        weights.yf_wait(k)
    weights.xz_wait(4)
    feed.swap_down()
    feed.over_wait(0)
    feed.hidden(0)
    feed.rows_rest()
    feed.over_wait(1)
    feed.hidden(1)
    feed.over_wait(-1)
    feed.hidden(-1)
    feed.swapped_down()
    feed.down(1)
    feed.down(-1)
    feed.second.send_near()
    feed.rows_far()
    feed.over_wait(2)
    feed.hidden(2)
    feed.down(2)
    feed.second.send_far()
    feed.down(0)
    feed.second.join()
    feed.finish()
    net.drain()


def per_device(
    residual,
    first_group_queries,
    first_group_keys,
    second_group_queries,
    second_group_keys,
    primary_retain_switch_inputs,
    secondary_retain_switch_inputs,
    timestep_fading_exponent,
    values,
    output_gate_logits,
    head_norm_gains,
    output_projection,
    feedforward_norm_gain,
    gate_projection,
    up_projection,
    down_projection,
):
    w = jnp.concatenate([gate_projection, down_projection.T, up_projection], axis=0)
    args = (
        residual,
        first_group_queries,
        first_group_keys,
        second_group_queries,
        second_group_keys,
        primary_retain_switch_inputs,
        secondary_retain_switch_inputs,
        timestep_fading_exponent.reshape(NCH, CH),
        values,
        output_gate_logits,
        head_norm_gains,
        output_projection,
        feedforward_norm_gain.reshape(1, -1),
        w,
    )
    return pl.pallas_call(
        kernel,
        out_shape=jax.ShapeDtypeStruct(residual.shape, BF16),
        in_specs=[pl.BlockSpec(memory_space=pltpu.VMEM)] * len(args),
        out_specs=pl.BlockSpec(memory_space=pltpu.VMEM),
        scratch_shapes=[pltpu.VMEM(shape, dtype) for shape, dtype in SCRATCH.values()]
        + [
            pltpu.SemaphoreType.DMA,
            pltpu.SemaphoreType.DMA((COPIES,)),
            pltpu.SemaphoreType.DMA((COPIES,)),
        ],
        compiler_params=pltpu.CompilerParams(
            collective_id=0, has_side_effects=True, vmem_limit_bytes=66000000
        ),
    )(*args)


def solution(mesh):
    finer = Mesh(mesh.devices.reshape(NZ, NY, NX, 2), SP_TP)
    return jax.shard_map(
        per_device,
        mesh=finer,
        in_specs=(
            P(SP_TP, None),
            P(SP, TP),
            P(SP, TP),
            P(SP, TP),
            P(SP, TP),
            P(SP, TP),
            P(SP, TP),
            P(SP),
            P(None, SP, TP),
            P(None, SP, TP),
            P(None, TP),
            P(None, TP, None),
            P(),
            P(SP, TP),
            P(SP, TP),
            P(TP, SP),
        ),
        out_specs=P(SP_TP, None),
        check_vma=False,
    )
```

```python
import functools

import jax
import jax.numpy as jnp
from jax import lax
from jax.experimental import pallas as pl
from jax.experimental.pallas import tpu as pltpu
from jax.sharding import Mesh
from jax.sharding import PartitionSpec as P

SP = ("sp_0", "sp_1")
TP = ("tp_0", "tp_1")
SP_TP = ("sp_0", "sp_1", "tp_0", "tp_1")
EPS = 1e-06
MESH = pl.DeviceIdType.MESH
BF16, F32 = jnp.bfloat16, jnp.float32

NZ, NY, NX = 8, 4, 4
CH = 128
NCH = 8
KA, KB = 128, 64
FF = 768
WR = 192
UP, DOWN = 64, 128
DT = (((1,), (1,)), ((), ()))
TD = (((0,), (0,)), ((), ()))


def dot(a, b):
    return jnp.dot(a, b, preferred_element_type=F32)


def dotg(a, b, dims):
    return lax.dot_general(a, b, dims, preferred_element_type=F32)


class Net:
    def __init__(self, ssem, rsem):
        self.ssem, self.rsem = ssem, rsem
        self.z, self.y = lax.axis_index("sp_0"), lax.axis_index("sp_1")
        self.x, self.c = lax.axis_index("tp_0"), lax.axis_index("tp_1")
        self.count = 0
        self.sent = []

    def number(self):
        self.count += 1
        return self.count - 1

    def at_z(self, k):
        return lax.rem(self.z + (k + NZ), NZ)

    def at_y(self, k):
        return lax.rem(self.y + (k + NY), NY)

    def at_x(self, k):
        return lax.rem(self.x + (k + NX), NX)

    def to_z(self, k):
        return (self.at_z(k), self.y, self.x, self.c)

    def to_y(self, k):
        return (self.z, self.at_y(k), self.x, self.c)

    def to_x(self, k):
        return (self.z, self.y, self.at_x(k), self.c)

    def partner(self):
        return (self.z, self.y, self.x, 1 - self.c)

    def _copy(self, src, dst, number, device):
        return pltpu.make_async_remote_copy(
            src_ref=src,
            dst_ref=dst,
            send_sem=self.ssem.at[number],
            recv_sem=self.rsem.at[number],
            device_id=device,
            device_id_type=MESH,
        )

    def send(self, src, dst, number, device):
        copy = self._copy(src, dst, number, device)
        copy.start()
        self.sent.append(copy)

    def arrived(self, dst, number):
        self._copy(dst, dst, number, self.partner()).wait_recv()

    def drain(self):
        for copy in self.sent:
            copy.wait_send()

    def greet(self):
        peers = [self.to_z(k) for k in (4, 3, -3, 2, -2, 1, -1)]
        peers += [self.to_y(k) for k in (2, 1, -1)]
        peers += [self.to_x(k) for k in (1, -1)]
        peers += [self.partner()]
        self.peers = len(peers)
        barrier = pltpu.get_barrier_semaphore()
        for device in peers:
            pl.semaphore_signal(barrier, inc=1, device_id=device, device_id_type=MESH)

    def greeted(self):
        pl.semaphore_wait(pltpu.get_barrier_semaphore(), self.peers)


class Weights:
    def __init__(self, net, wg):
        self.net, self.wg = net, wg
        n = net.number
        self.xb = [n(), n()]
        self.xf = [n(), n()]
        self.xz = [[n(), n()] for _ in range(NZ // 2)]
        self.yz = [[n(), n()] for _ in range(NZ // 2)]
        self.yb = {u: [[n(), n()] for _ in range(NZ)] for u in (UP, DOWN)}
        self.yf = {u: [[n(), n()] for _ in range(NZ)] for u in (UP, DOWN)}

    def slot(self, kz, ky, lo, hi):
        return self.wg.at[self.net.at_z(kz), self.net.at_y(ky), lo:hi]

    def x_out(self):
        net = self.net
        for d, k in enumerate((1, -1)):
            part = self.slot(0, 0, 0, 64)
            net.send(part, part, self.xb[d], net.to_y(k))

    def x_forward(self):
        net = self.net
        for d, (k, lo, hi) in enumerate(((1, 0, 32), (-1, 32, 64))):
            net.arrived(self.slot(0, -k, 0, 64), self.xb[d])
            part = self.slot(0, -k, lo, hi)
            net.send(part, part, self.xf[d], net.to_y(k))

    def x_forwarded(self):
        for d, (lo, hi) in enumerate(((0, 32), (32, 64))):
            self.net.arrived(self.slot(0, 2, lo, hi), self.xf[d])

    def x_bundle(self, kz, s, d):
        lo, hi = (0, NY) if s < NZ // 2 else ((0, NY // 2) if d == 0 else (NY // 2, NY))
        return self.wg.at[self.net.at_z(kz), lo:hi, 0:64]

    def xz_send(self, s):
        for d, k in enumerate((1, -1)):
            part = self.x_bundle(-k * (s - 1), s, d)
            self.net.send(part, part, self.xz[s - 1][d], self.net.to_z(k))

    def xz_wait(self, s):
        for d, k in enumerate((1, -1)):
            self.net.arrived(self.x_bundle(-k * s, s, d), self.xz[s - 1][d])

    def y_rows(self, s, d):
        return (64, 192) if s < NZ // 2 else ((64, 128) if d == 0 else (128, 192))

    def yz_send(self, s):
        net = self.net
        for d, k in enumerate((1, -1)):
            part = self.slot(-k * (s - 1), 0, *self.y_rows(s, d))
            net.send(part, part, self.yz[s - 1][d], net.to_z(k))

    def yz_wait(self, s):
        for d, k in enumerate((1, -1)):
            self.net.arrived(self.slot(-k * s, 0, *self.y_rows(s, d)), self.yz[s - 1][d])

    def yb_send(self, lo, *kzs):
        net = self.net
        for kz in kzs:
            part = self.slot(kz, 0, lo, lo + 64)
            for d, k in enumerate((1, -1)):
                net.send(part, part, self.yb[lo][kz % NZ][d], net.to_y(k))

    def yf_send(self, lo, *kzs):
        net = self.net
        for kz in kzs:
            for d, k in enumerate((1, -1)):
                net.arrived(self.slot(kz, -k, lo, lo + 64), self.yb[lo][kz % NZ][d])
                part = self.slot(kz, -k, lo + 32 * d, lo + 32 * d + 32)
                net.send(part, part, self.yf[lo][kz % NZ][d], net.to_y(k))

    def yf_wait(self, lo, *kzs):
        for kz in kzs:
            for d in range(2):
                part = self.slot(kz, 2, lo + 32 * d, lo + 32 * d + 32)
                self.net.arrived(part, self.yf[lo][kz % NZ][d])


def rows_of(chunk, size=CH):
    return pl.ds(pl.multiple_of(chunk * size, size), size)


def iotas(n):
    return (
        lax.broadcasted_iota(jnp.int32, (n, n), 0),
        lax.broadcasted_iota(jnp.int32, (n, n), 1),
    )


class Attention:
    def __init__(self, net, r):
        self.net, self.r = net, r
        n = net.number
        self.m1 = [n() for _ in range(NY)]
        self.m2 = [n() for _ in range(NZ)]
        self.m3 = [n() for _ in range(NY)]
        self.heads = (
            (KA, r["ba"], r["sa"], r["ea"], r["pa"], r["ta"], 0),
            (KB, r["bb"], r["sb"], r["eb"], r["pb"], r["tb"], 1),
        )

    def load(self, kind, h, rows):
        if h == 0:
            return self.r[kind + "a"][rows, :].astype(F32)
        return self.r[kind + "b"][:, rows].astype(F32).T

    def states(self):
        r = self.r
        row, col = iotas(CH)
        lower = row >= col
        tri = jnp.where(lower, 1.0, 0.0).astype(BF16)
        tri2 = jnp.concatenate([tri, tri], axis=1)

        def step(c, carry):
            rows = rows_of(c)
            line = r["fade"][pl.ds(c, 1), :]
            fade = jnp.sum(jnp.where(lower, line, 0.0), axis=1, keepdims=True)
            new = []
            for (width, b, s, e, p, t, h), (state, before) in zip(self.heads, carry):
                x = self.load("g", h, rows)
                slow = (jnp.minimum(x, 0.0) - jnp.log1p(jnp.exp(-jnp.abs(x)))) * (1.0 / 16.0)
                high = slow.astype(BF16)
                low = (slow - high.astype(F32)).astype(BF16)
                sums = dot(tri2, jnp.concatenate([high, low], axis=0)) + fade
                b[rows, :] = sums
                total = sums[CH - 1 : CH, :]
                faded = (self.load("k", h, rows) * jnp.exp(total - sums)).astype(BF16)
                s[c] = state
                e[pl.ds(c, 1), :] = before
                state = jnp.exp(total) * state + dotg(r["v"][h, rows, :], faded, TD)
                new.append((state, before + total))
            return tuple(new)

        zero = tuple(
            (jnp.zeros((CH, width), F32), jnp.zeros((1, width), F32)) for width in (KA, KB)
        )
        (state_a, log_a), (state_b, log_b) = lax.fori_loop(0, NCH, step, zero, unroll=4)
        out = r["m1s"]
        quarter = CH // NY
        row16 = lax.broadcasted_iota(jnp.int32, (16, 1), 0)

        def two_rows(value):
            high = value.astype(BF16).astype(F32)
            return jnp.where(row16 == 0, high, value - high).astype(BF16)

        ends_a, ends_b = two_rows(jnp.exp(log_a)), two_rows(jnp.exp(log_b))
        for i in range(NY):
            part = slice(i * quarter, (i + 1) * quarter)
            out[i, 0:quarter, 0:KA] = state_a[part].astype(BF16)
            out[i, 0:quarter, KA : KA + KB] = state_b[part].astype(BF16)
            out[i, 0:quarter, KA + KB :] = jnp.zeros((quarter, KB), BF16)
            out[i, quarter:, 0:KA] = ends_a
            out[i, quarter:, KA : KA + KB] = ends_b
            out[i, quarter:, KA + KB :] = jnp.zeros((16, KB), BF16)

    def send_quarters(self):
        net, r = self.net, self.r
        for k in range(1, NY):
            net.send(r["m1s"].at[net.at_y(k)], r["m1r"].at[k], self.m1[k], net.to_y(k))

    @staticmethod
    def opened(message):
        quarter = CH // NY
        state = message[0:quarter, :].astype(F32)
        decay = message[quarter : quarter + 1, :].astype(F32) + message[
            quarter + 1 : quarter + 2, :
        ].astype(F32)
        return state, decay

    def send_line_total(self):
        net, r = self.net, self.r
        quarter = CH // NY
        for k in range(1, NY):
            net.arrived(r["m1r"].at[k], self.m1[k])
        r["m1r"][0] = r["m1s"][net.y]
        state = jnp.zeros((quarter, 256), F32)
        decay = jnp.ones((1, 256), F32)
        for i in range(NY):
            slot = lax.rem(net.y - i + NY, NY)
            own, factor = self.opened(r["m1r"][slot])
            state, decay = factor * state + own, factor * decay
        row16 = lax.broadcasted_iota(jnp.int32, (16, 1), 0)
        high = decay.astype(BF16).astype(F32)
        r["m2s"][0:quarter, :] = state.astype(BF16)
        r["m2s"][quarter:, :] = jnp.where(row16 == 0, high, decay - high).astype(BF16)
        for k in (1, -1, 2, -2, 3, -3, 4):
            net.send(r["m2s"], r["m2r"].at[k % NZ], self.m2[k % NZ], net.to_z(k))

    def send_incoming(self):
        net, r = self.net, self.r
        quarter = CH // NY
        for k in range(1, NZ):
            net.arrived(r["m2r"].at[k], self.m2[k])
        r["m2r"][0] = jnp.zeros((48, 256), BF16)
        state = jnp.zeros((quarter, 256), F32)
        for i in range(NZ - 1):
            slot = lax.rem(net.z - i + NZ, NZ)
            own, factor = self.opened(r["m2r"][slot])
            state = jnp.where(i < net.z, factor * state + own, state)
        for i in range(NY):
            r["m3s"][i] = state.astype(BF16)
            slot = lax.rem(net.y - i + NY, NY)
            own, factor = self.opened(r["m1r"][slot])
            state = factor * state + own
        for k in range(1, NY):
            net.send(r["m3s"].at[net.at_y(k)], r["m3r"].at[net.y], self.m3[k], net.to_y(k))
        r["m3r"][net.y] = r["m3s"][net.y]

    def incoming(self):
        net, r = self.net, self.r
        for k in range(1, NY):
            net.arrived(r["m3r"].at[net.at_y(-k)], self.m3[k])

    def scores(self, start, stop):
        r = self.r
        row, col = iotas(CH)
        near = ((row >> 5) == (col >> 5)) & (row >= col)
        middle = ((row >> 6) == (col >> 6)) & ((row >> 5) > (col >> 5))
        far = (row >> 6) > (col >> 6)

        def around(sums, size, at):
            width = sums.shape[1]
            parts = sums.reshape(CH // size, size, width)
            return (parts - parts[:, at : at + 1, :]).reshape(CH, width)

        def step(c, carry):
            rows = rows_of(c)
            for width, b, s, e, p, t, h in self.heads:
                sums = b[rows, :]
                query = self.load("q", h, rows) * (width**-0.5)
                key = self.load("k", h, rows)
                t[rows, :] = (query * jnp.exp(sums)).astype(BF16)
                at = around(sums, 32, 15)
                local = dotg(
                    (query * jnp.exp(at)).astype(BF16), (key * jnp.exp(-at)).astype(BF16), DT
                )
                total = jnp.where(near, local, 0.0)
                for size, at, mask in ((64, 31, middle), (128, 63, far)):
                    f = jnp.exp(-jnp.abs(around(sums, size, at)))
                    wide = dotg((query * f).astype(BF16), (key * f).astype(BF16), DT)
                    total = jnp.where(mask, wide, total)
                p[c] = total.astype(BF16)
            return carry

        lax.fori_loop(start, stop, step, 0, unroll=4)

    def gated(self, first, count):
        r = self.r

        def step(i, carry):
            c = first + i
            rows = rows_of(c)
            before_state = r["m3r"][...].astype(F32).reshape(CH, 256)
            for width, b, s, e, p, t, h in self.heads:
                state = s[c] + jnp.exp(e[pl.ds(c, 1), :]) * before_state[:, h * KA : h * KA + width]
                out = dot(p[c], r["v"][h, rows, :]) + dotg(t[rows, :], state.astype(BF16), DT)
                inverse = lax.rsqrt(jnp.mean(out * out, axis=-1, keepdims=True) + EPS)
                gate = r["og"][h, rows, :].astype(F32)
                normed = out * inverse * r["gain"][h : h + 1, :]
                value = gate * jax.nn.sigmoid(gate) * normed
                r["gat"][rows, h * CH : (h + 1) * CH] = value.astype(BF16)
            return carry

        lax.fori_loop(0, count, step, 0, unroll=2)


HALF = 1024
BLK = 256
LEFT, RIGHT = slice(0, 512), slice(512, 1024)


class Reduce:
    def __init__(self, net, part, comb, hop, joined, direct):
        self.net, self.part, self.comb = net, part, comb
        self.hop, self.joined, self.direct = hop, joined, direct
        n = net.number
        self.h = [[n(), n()] for _ in range(2)]
        self.j = [[n(), n()] for _ in range(2)]
        self.d = [[n(), n()] for _ in range(2)]

    def send_far(self, *pieces):
        net = self.net
        for piece in pieces:
            rows = pl.ds(piece * CH, CH)
            for side, (k, cols) in enumerate(((1, LEFT), (-1, RIGHT))):
                net.send(
                    self.part.at[0, rows, cols],
                    self.hop.at[side, rows],
                    self.h[side][piece],
                    net.to_x(k),
                )

    def send_near(self, *pieces):
        net = self.net
        for piece in pieces:
            rows = pl.ds(piece * CH, CH)
            for side, (k, block, cols) in enumerate(((1, 1, RIGHT), (-1, 2, LEFT))):
                net.send(
                    self.part.at[block, rows, cols],
                    self.direct.at[side, rows],
                    self.d[side][piece],
                    net.to_x(k),
                )

    def join(self, *pieces):
        net = self.net
        for piece in pieces:
            rows = slice(piece * CH, (piece + 1) * CH)
            for side, (k, block, cols) in enumerate(((1, 1, LEFT), (-1, 2, RIGHT))):
                net.arrived(self.hop.at[side, rows], self.h[side][piece])
                both = self.part[block, rows, cols].astype(F32) + self.hop[side, rows, :].astype(
                    F32
                )
                self.comb[side, rows, :] = both.astype(BF16)
                net.send(
                    self.comb.at[side, rows],
                    self.joined.at[side, rows],
                    self.j[side][piece],
                    net.to_x(k),
                )

    def arrived(self, piece):
        net = self.net
        rows = slice(piece * CH, (piece + 1) * CH)
        for side in range(2):
            net.arrived(self.direct.at[side, rows], self.d[side][piece])
            net.arrived(self.joined.at[side, rows], self.j[side][piece])

    def total(self, own, rows):
        left = (
            own[rows, LEFT]
            + self.joined[0, rows, :].astype(F32)
            + self.direct[1, rows, :].astype(F32)
        )
        right = (
            own[rows, RIGHT]
            + self.joined[1, rows, :].astype(F32)
            + self.direct[0, rows, :].astype(F32)
        )
        return left, right


class Feed:
    def __init__(self, net, r):
        self.net, self.r = net, r
        n = net.number
        self.n_res, self.n_wo, self.n_out = n(), n(), n()
        self.n_ss = [n(), n()]
        self.n_dp = [n() for _ in range(4)]
        self.n_gat = [n() for _ in range(NX)]
        self.n_hid = [[n(), n()] for _ in range(NX)]
        self.ring = [[n(), n()] for _ in range(2)]
        self.far = [[n(), n()] for _ in range(2)]
        self.over = [[n(), n()] for _ in range(NX)]
        self.first = Reduce(net, r["p1"], r["c1"], r["h1"], r["j1"], r["d1"])
        self.second = Reduce(net, r["p2"], r["c2"], r["h2"], r["j2"], r["d2"])

    def cols(self, core):
        return pl.ds(pl.multiple_of(core * HALF, HALF), HALF)

    def block(self, k):
        return rows_of(self.net.at_x(k), BLK)

    def swap_inputs(self):
        net, r = self.net, self.r
        other = 1 - net.c
        net.send(
            r["res"].at[:, self.cols(other)], r["base"].at[net.c], self.n_res, net.partner()
        )
        net.send(r["wo"].at[:, :, self.cols(other)], r["wop"], self.n_wo, net.partner())

    def send_gated(self, k):
        net, r = self.net, self.r
        rows = self.block(k)
        net.send(r["gat"].at[rows], r["gatp"].at[rows], self.n_gat[k % NX], net.partner())

    def swapped_inputs(self):
        net, r = self.net, self.r
        net.arrived(r["wop"], self.n_wo)
        net.arrived(r["base"].at[1 - net.c], self.n_res)
        r["base"][net.c] = r["res"][:, self.cols(net.c)]

    def project(self, k):
        net, r = self.net, self.r
        rows = self.block(k)
        net.arrived(r["gatp"].at[rows], self.n_gat[k % NX])
        mine, theirs = r["gat"][rows, :], r["gatp"][rows, :]
        for side in range(2):
            cols = slice(side * 512, (side + 1) * 512)
            at = pl.ds(pl.multiple_of(net.c * HALF + side * 512, 512), 512)
            part = dot(mine, r["wo"][:, :, at].reshape(2 * CH, 512)) + dot(
                theirs, r["wop"][:, :, cols].reshape(2 * CH, 512)
            )
            if k == 0:
                r["own1"][:, cols] = part
            else:
                r["p1"][{2: 0, 1: 1, -1: 2}[k], :, cols] = part.astype(BF16)

    def middle(self, piece):
        net, r = self.net, self.r
        self.first.arrived(piece)
        rows = slice(piece * CH, (piece + 1) * CH)
        left, right = self.first.total(r["own1"], rows)
        base = r["base"].at[piece]
        mid_l = (base[:, LEFT].astype(F32) + left).astype(BF16)
        mid_r = (base[:, RIGHT].astype(F32) + right).astype(BF16)
        r["mid"][rows, LEFT] = mid_l
        r["mid"][rows, RIGHT] = mid_r
        mid_l, mid_r = mid_l.astype(F32), mid_r.astype(F32)
        squares = jnp.sum(mid_l * mid_l + mid_r * mid_r, axis=-1, keepdims=True)
        r["ss"][piece] = jnp.broadcast_to(squares, (CH, 128))
        net.send(r["ss"].at[piece], r["ssp"].at[piece], self.n_ss[piece], net.partner())
        net.arrived(r["ssp"].at[piece], self.n_ss[piece])
        inverse = lax.rsqrt((squares + r["ssp"][piece][:, 0:1]) * (1.0 / 2048.0) + EPS)
        gain = r["fgain"][:, self.cols(net.c)]
        start = pl.multiple_of(net.x * BLK + piece * CH, CH)
        for side, mid in ((LEFT, mid_l), (RIGHT, mid_r)):
            normed = (mid * inverse * gain[:, side]).astype(BF16)
            r["all"][net.c, pl.ds(start, CH), side] = normed

    def piece(self, k, half, side=slice(0, HALF), other=False):
        start = pl.multiple_of(self.net.at_x(k) * BLK + half * CH, CH)
        core = 1 - self.net.c if other else self.net.c
        return self.r["all"].at[core, pl.ds(start, CH), side]

    def over_send(self, k, half):
        part = self.piece(k, half)
        self.net.send(part, part, self.over[k % NX][half], self.net.partner())

    def over_wait(self, *pieces):
        for k, half in pieces:
            self.net.arrived(self.piece(k, half, other=True), self.over[k % NX][half])

    def rows_out(self, half):
        net = self.net
        part = self.piece(0, half)
        for d, k in enumerate((1, -1)):
            net.send(part, part, self.ring[d][half], net.to_x(k))
        self.over_send(0, half)

    def rows_on(self, half):
        net = self.net
        for d, (k, side) in enumerate(((1, LEFT), (-1, RIGHT))):
            net.arrived(self.piece(-k, half), self.ring[d][half])
            part = self.piece(-k, half, side)
            net.send(part, part, self.far[d][half], net.to_x(k))
            self.over_send(-k, half)

    def rows_far(self, half):
        for d, side in enumerate((LEFT, RIGHT)):
            self.net.arrived(self.piece(2, half, side), self.far[d][half])
        self.over_send(2, half)

    def rows(self, k, half):
        start = pl.multiple_of(self.net.at_x(k) * BLK + half * CH, CH)
        return pl.ds(start, CH)

    def hidden(self, *pieces):
        net, r = self.net, self.r
        self.over_wait(*pieces)
        blocks = [self.rows(*piece) for piece in pieces]

        def step(n, carry):
            at = pl.ds(pl.multiple_of(n * 256, 256), 256)
            lines = jnp.concatenate(
                [
                    jnp.concatenate([r["all"][0, rows, :], r["all"][1, rows, :]], axis=1)
                    for rows in blocks
                ],
                axis=0,
            )
            gate, up = (
                dot(lines, r["wg"][:, :, low : low + 64, at].reshape(2 * HALF, 256))
                for low in (0, UP)
            )
            value = (gate * jax.nn.sigmoid(gate) * up).astype(BF16)
            for i, rows in enumerate(blocks):
                r["hid"][rows, at] = value[i * CH : (i + 1) * CH]
            return carry

        lax.fori_loop(0, FF // 256, step, 0)
        for (k, half), rows in zip(pieces, blocks):
            net.send(
                r["hid"].at[rows], r["hidp"].at[rows], self.n_hid[k % NX][half], net.partner()
            )

    def swap_tile(self, kz):
        net, r = self.net, self.r
        z = net.at_z(kz)

        @pl.when(z // 4 == 1 - net.c)
        def _():
            n = lax.rem(z, 4)
            self.tile(z, n).start()

    def tile(self, z, n):
        r = self.r
        return self.net._copy(
            r["wg"].at[z, :, DOWN:], r["dp"].at[n], self.n_dp[0] + n, self.net.partner()
        )

    def swapped_down(self):
        for n in range(4):
            copy = self.tile(4 * (1 - self.net.c) + n, n)
            copy.wait_send()
            copy.wait_recv()

    def down(self, *pieces):
        net, r = self.net, self.r
        blocks = [self.rows(*piece) for piece in pieces]
        for (k, half), rows in zip(pieces, blocks):
            net.arrived(r["hidp"].at[rows], self.n_hid[k % NX][half])

        def step(n, carry):
            at = pl.ds(pl.multiple_of(n * 256, 256), 256)
            lines = jnp.concatenate(
                [
                    jnp.concatenate([r["hid"][rows, :], r["hidp"][rows, :]], axis=1)
                    for rows in blocks
                ],
                axis=0,
            )
            w = jnp.concatenate(
                [
                    r["wg"][4 * net.c + n, :, DOWN:, :].reshape(256, FF),
                    r["dp"][n].reshape(256, FF),
                ],
                axis=1,
            )
            part = dotg(lines, w, DT)
            for i, (k, half) in enumerate(pieces):
                mine = part[i * CH : (i + 1) * CH]
                rows = slice(half * CH, (half + 1) * CH)
                if k == 0:
                    r["own2"][rows, at] = mine
                else:
                    r["p2"][{2: 0, 1: 1, -1: 2}[k], rows, at] = mine.astype(BF16)
            return carry

        lax.fori_loop(0, HALF // 256, step, 0)

    def finish(self):
        net, r = self.net, self.r
        for piece in range(2):
            self.second.arrived(piece)
            rows = slice(piece * CH, (piece + 1) * CH)
            left, right = self.second.total(r["own2"], rows)
            r["outs"][piece, :, LEFT] = (r["mid"][rows, LEFT].astype(F32) + left).astype(BF16)
            r["outs"][piece, :, RIGHT] = (r["mid"][rows, RIGHT].astype(F32) + right).astype(BF16)
        net.send(r["outs"].at[1 - net.c], r["outp"], self.n_out, net.partner())

        @pl.when(net.c == 0)
        def _():
            r["lo"][...] = r["outs"][0]

        @pl.when(net.c == 1)
        def _():
            r["hi"][...] = r["outs"][1]

        net.arrived(r["outp"], self.n_out)

        @pl.when(net.c == 0)
        def _():
            r["hi"][...] = r["outp"][...]

        @pl.when(net.c == 1)
        def _():
            r["lo"][...] = r["outp"][...]


INPUTS = dict(
    ga=((1024, KA), BF16),
    gb=((KB, 1024), BF16),
    fade=((NCH, CH), F32),
    ka=((1024, KA), BF16),
    kb=((KB, 1024), BF16),
    v=((2, 1024, CH), BF16),
    gate=None,
    down=None,
    up=None,
    qa=((1024, KA), BF16),
    qb=((KB, 1024), BF16),
    res=((CH, 2048), BF16),
    wo=((2, CH, 2048), BF16),
    og=((2, 1024, CH), BF16),
    gain=((2, CH), F32),
    fgain=((1, 2048), F32),
)
SCRATCH = dict(
    wg=((NZ, NY, WR, FF), BF16),
    ba=((1024, KA), F32),
    bb=((1024, KB), F32),
    sa=((NCH, CH, KA), F32),
    sb=((NCH, CH, KB), F32),
    ea=((NCH, KA), F32),
    eb=((NCH, KB), F32),
    pa=((NCH, CH, CH), BF16),
    pb=((NCH, CH, CH), BF16),
    ta=((1024, KA), BF16),
    tb=((1024, KB), BF16),
    m1s=((NY, 48, 256), BF16),
    m1r=((NY, 48, 256), BF16),
    m2s=((48, 256), BF16),
    m2r=((NZ, 48, 256), BF16),
    m3s=((NY, 32, 256), BF16),
    m3r=((NY, 32, 256), BF16),
    gat=((1024, 256), BF16),
    gatp=((1024, 256), BF16),
    wop=((2, CH, HALF), BF16),
    base=((2, CH, HALF), BF16),
    own1=((BLK, HALF), F32),
    p1=((3, BLK, HALF), BF16),
    c1=((2, BLK, 512), BF16),
    h1=((2, BLK, 512), BF16),
    j1=((2, BLK, 512), BF16),
    d1=((2, BLK, 512), BF16),
    mid=((BLK, HALF), BF16),
    ss=((2, CH, 128), F32),
    ssp=((2, CH, 128), F32),
    all=((2, 1024, HALF), BF16),
    hid=((1024, FF), BF16),
    hidp=((1024, FF), BF16),
    dp=((4, NY, 64, FF), BF16),
    own2=((BLK, HALF), F32),
    p2=((3, BLK, HALF), BF16),
    c2=((2, BLK, 512), BF16),
    h2=((2, BLK, 512), BF16),
    j2=((2, BLK, 512), BF16),
    d2=((2, BLK, 512), BF16),
    outs=((2, CH, HALF), BF16),
    outp=((CH, HALF), BF16),
)
COPIES = 192


class Inputs:
    def __init__(self, net, r, given, sems):
        self.copies = {}
        for i, name in enumerate(INPUTS):
            if INPUTS[name] is None:
                lo = {"gate": 0, "up": UP, "down": DOWN}[name]
                dst = r["wg"].at[net.z, net.y, lo : lo + 64]
            else:
                dst = r[name]
            self.copies[name] = pltpu.make_async_copy(given[name], dst, sems.at[i])

    def fetch(self, *names):
        for name in names:
            self.copies[name].start()

    def ready(self, *names):
        for name in names:
            self.copies[name].wait()


def kernel(*refs):
    count = len(INPUTS)
    given = dict(zip(INPUTS, refs))
    held = [name for name in INPUTS if INPUTS[name] is not None]
    r = dict(zip(["lo", "hi"] + list(SCRATCH) + held, refs[count:]))
    isem, ssem, rsem = refs[-3:]
    net = Net(ssem, rsem)
    weights = Weights(net, r["wg"])
    attention = Attention(net, r)
    feed = Feed(net, r)
    assert net.count <= COPIES, net.count
    inputs = Inputs(net, r, given, isem)
    inputs.fetch("ga", "gb", "fade", "ka", "kb", "v")
    net.greet()
    inputs.ready("ga", "gb", "fade", "ka", "kb", "v")
    inputs.fetch("gate", "up", "down", "qa", "qb", "res", "wo", "og", "gain", "fgain")
    attention.states()
    inputs.ready("gate", "up", "down", "qa", "qb", "res", "wo", "og", "gain", "fgain")
    net.greeted()
    attention.send_quarters()
    weights.yz_send(1)
    weights.x_out()
    weights.yb_send(UP, 0)
    feed.swap_inputs()
    attention.scores(0, 8)
    attention.send_line_total()
    weights.x_forward()
    weights.yb_send(DOWN, 0)
    weights.yz_wait(1)
    weights.yz_send(2)
    weights.yb_send(UP, 1, -1)
    weights.x_forwarded()
    weights.xz_send(1)
    feed.swapped_inputs()
    attention.send_incoming()
    attention.incoming()
    for k in (2, 1, -1, 0):
        attention.gated(2 * net.at_x(k), 2)
        feed.send_gated(k)
        if k == 1:
            feed.project(2)
            feed.first.send_far(0, 1)
    feed.project(1)
    feed.project(-1)
    feed.first.send_near(0, 1)
    feed.project(0)
    weights.yz_wait(2)
    weights.yz_send(3)
    weights.yb_send(UP, 2, -2)
    weights.yf_send(UP, 0, 1, -1)
    weights.yb_send(DOWN, 1, -1)
    weights.xz_wait(1)
    weights.xz_send(2)
    weights.yz_wait(3)
    weights.yz_send(4)
    weights.yb_send(UP, 3, -3)
    weights.yb_send(DOWN, 2, -2)
    feed.first.join(0, 1)
    weights.yf_send(UP, 2, -2)
    weights.xz_wait(2)
    weights.xz_send(3)
    weights.yz_wait(4)
    weights.yb_send(UP, 4)
    weights.yb_send(DOWN, 3, -3, 4)
    feed.middle(0)
    feed.rows_out(0)
    feed.middle(1)
    feed.rows_out(1)
    feed.rows_on(0)
    weights.yf_send(UP, 3, -3)
    weights.xz_wait(3)
    weights.xz_send(4)
    feed.rows_on(1)
    weights.yf_send(UP, 4)
    weights.yf_send(DOWN, 0, 1, -1, 2, -2, 3, -3)
    weights.xz_wait(4)
    weights.yf_wait(UP, 0, 1, -1, 2, -2, 3, -3, 4)
    feed.hidden((1, 0), (-1, 0))
    weights.yf_send(DOWN, 4)
    feed.hidden((1, 1), (-1, 1))
    feed.rows_far(0)
    for k in (0, 1, -1, 2, -2, 3, -3, 4):
        weights.yf_wait(DOWN, k)
        feed.swap_tile(k)
    feed.swapped_down()
    feed.down((1, 0), (-1, 0))
    feed.second.send_near(0)
    feed.down((1, 1), (-1, 1))
    feed.second.send_near(1)
    feed.rows_far(1)
    feed.hidden((2, 0), (2, 1))
    feed.hidden((0, 0), (0, 1))
    feed.down((2, 0), (2, 1))
    feed.second.send_far(0, 1)
    feed.down((0, 0), (0, 1))
    feed.second.join(0, 1)
    feed.finish()
    net.drain()


def per_device(
    residual,
    first_group_queries,
    first_group_keys,
    second_group_queries,
    second_group_keys,
    primary_retain_switch_inputs,
    secondary_retain_switch_inputs,
    timestep_fading_exponent,
    values,
    output_gate_logits,
    head_norm_gains,
    output_projection,
    feedforward_norm_gain,
    gate_projection,
    up_projection,
    down_projection,
):
    given = dict(
        ga=primary_retain_switch_inputs,
        gb=secondary_retain_switch_inputs.T,
        fade=timestep_fading_exponent.reshape(NCH, CH),
        ka=first_group_keys,
        kb=second_group_keys.T,
        v=values,
        gate=gate_projection,
        down=down_projection.T,
        up=up_projection,
        qa=first_group_queries,
        qb=second_group_queries.T,
        res=residual,
        wo=output_projection,
        og=output_gate_logits,
        gain=head_norm_gains,
        fgain=feedforward_norm_gain.reshape(1, -1),
    )
    half = jax.ShapeDtypeStruct((CH, HALF), BF16)
    buffers = list(SCRATCH.values()) + [spec for spec in INPUTS.values() if spec is not None]
    lo, hi = pl.pallas_call(
        kernel,
        out_shape=(half, half),
        in_specs=[pl.BlockSpec(memory_space=pl.ANY)] * len(INPUTS),
        out_specs=(pl.BlockSpec(memory_space=pltpu.VMEM),) * 2,
        scratch_shapes=[pltpu.VMEM(shape, dtype) for shape, dtype in buffers]
        + [
            pltpu.SemaphoreType.DMA((len(INPUTS),)),
            pltpu.SemaphoreType.DMA((COPIES,)),
            pltpu.SemaphoreType.DMA((COPIES,)),
        ],
        compiler_params=pltpu.CompilerParams(
            collective_id=0, has_side_effects=True, vmem_limit_bytes=66000000
        ),
    )(*(given[name] for name in INPUTS))
    return jnp.concatenate([lo, hi], axis=1)


def solution(mesh):
    finer = Mesh(mesh.devices.reshape(NZ, NY, NX, 2), SP_TP)
    return jax.shard_map(
        per_device,
        mesh=finer,
        in_specs=(
            P(SP_TP, None),
            P(SP, TP),
            P(SP, TP),
            P(SP, TP),
            P(SP, TP),
            P(SP, TP),
            P(SP, TP),
            P(SP),
            P(None, SP, TP),
            P(None, SP, TP),
            P(None, TP),
            P(None, TP, None),
            P(),
            P(SP, TP),
            P(SP, TP),
            P(TP, SP),
        ),
        out_specs=P(SP_TP, None),
        check_vma=False,
    )
```

```python
import functools

import jax
import jax.numpy as jnp
from jax import lax
from jax.experimental import pallas as pl
from jax.experimental.pallas import tpu as pltpu
from jax.sharding import Mesh
from jax.sharding import PartitionSpec as P

SP = ("sp_0", "sp_1")
TP = ("tp_0", "tp_1")
SP_TP = ("sp_0", "sp_1", "tp_0", "tp_1")
EPS = 1e-06
MESH = pl.DeviceIdType.MESH
BF16, F32 = jnp.bfloat16, jnp.float32

NZ, NY, NX = 8, 4, 4
CH = 128
NCH = 8
KA, KB = 128, 64
FF = 768
WR = 192
UP, DOWN = 64, 128
DT = (((1,), (1,)), ((), ()))
TD = (((0,), (0,)), ((), ()))


def dot(a, b):
    return jnp.dot(a, b, preferred_element_type=F32)


def dotg(a, b, dims):
    return lax.dot_general(a, b, dims, preferred_element_type=F32)


class Net:
    def __init__(self, ssem, rsem):
        self.ssem, self.rsem = ssem, rsem
        self.z, self.y = lax.axis_index("sp_0"), lax.axis_index("sp_1")
        self.x, self.c = lax.axis_index("tp_0"), lax.axis_index("tp_1")
        self.count = 0
        self.sent = []

    def number(self):
        self.count += 1
        return self.count - 1

    def at_z(self, k):
        return lax.rem(self.z + (k + NZ), NZ)

    def at_y(self, k):
        return lax.rem(self.y + (k + NY), NY)

    def at_x(self, k):
        return lax.rem(self.x + (k + NX), NX)

    def to_z(self, k):
        return (self.at_z(k), self.y, self.x, self.c)

    def to_y(self, k):
        return (self.z, self.at_y(k), self.x, self.c)

    def to_x(self, k):
        return (self.z, self.y, self.at_x(k), self.c)

    def partner(self):
        return (self.z, self.y, self.x, 1 - self.c)

    def _copy(self, src, dst, number, device):
        return pltpu.make_async_remote_copy(
            src_ref=src,
            dst_ref=dst,
            send_sem=self.ssem.at[number],
            recv_sem=self.rsem.at[number],
            device_id=device,
            device_id_type=MESH,
        )

    def send(self, src, dst, number, device):
        copy = self._copy(src, dst, number, device)
        copy.start()
        self.sent.append(copy)

    def arrived(self, dst, number):
        self._copy(dst, dst, number, self.partner()).wait_recv()

    def drain(self):
        for copy in self.sent:
            copy.wait_send()

    def greet(self):
        peers = [self.to_z(k) for k in (4, 3, -3, 2, -2, 1, -1)]
        peers += [self.to_y(k) for k in (2, 1, -1)]
        peers += [self.to_x(k) for k in (1, -1)]
        peers += [self.partner()]
        self.peers = len(peers)
        barrier = pltpu.get_barrier_semaphore()
        for device in peers:
            pl.semaphore_signal(barrier, inc=1, device_id=device, device_id_type=MESH)

    def greeted(self):
        pl.semaphore_wait(pltpu.get_barrier_semaphore(), self.peers)


class Weights:
    def __init__(self, net, wg):
        self.net, self.wg = net, wg
        n = net.number
        self.xb = [n(), n()]
        self.xf = [n(), n()]
        self.xz = [[n(), n()] for _ in range(NZ // 2)]
        self.yz = [[n(), n()] for _ in range(NZ // 2)]
        self.yb = {u: [[n(), n()] for _ in range(NZ)] for u in (UP, DOWN)}
        self.yf = {u: [[n(), n()] for _ in range(NZ)] for u in (UP, DOWN)}

    def slot(self, kz, ky, lo, hi):
        return self.wg.at[self.net.at_z(kz), self.net.at_y(ky), lo:hi]

    def x_out(self):
        net = self.net
        for d, k in enumerate((1, -1)):
            part = self.slot(0, 0, 0, 64)
            net.send(part, part, self.xb[d], net.to_y(k))

    def x_forward(self):
        net = self.net
        for d, (k, lo, hi) in enumerate(((1, 0, 32), (-1, 32, 64))):
            net.arrived(self.slot(0, -k, 0, 64), self.xb[d])
            part = self.slot(0, -k, lo, hi)
            net.send(part, part, self.xf[d], net.to_y(k))

    def x_forwarded(self):
        for d, (lo, hi) in enumerate(((0, 32), (32, 64))):
            self.net.arrived(self.slot(0, 2, lo, hi), self.xf[d])

    def x_bundle(self, kz, s, d):
        lo, hi = (0, NY) if s < NZ // 2 else ((0, NY // 2) if d == 0 else (NY // 2, NY))
        return self.wg.at[self.net.at_z(kz), lo:hi, 0:64]

    def xz_send(self, s):
        for d, k in enumerate((1, -1)):
            part = self.x_bundle(-k * (s - 1), s, d)
            self.net.send(part, part, self.xz[s - 1][d], self.net.to_z(k))

    def xz_wait(self, s):
        for d, k in enumerate((1, -1)):
            self.net.arrived(self.x_bundle(-k * s, s, d), self.xz[s - 1][d])

    def y_rows(self, s, d):
        return (64, 192) if s < NZ // 2 else ((64, 128) if d == 0 else (128, 192))

    def yz_send(self, s):
        net = self.net
        for d, k in enumerate((1, -1)):
            part = self.slot(-k * (s - 1), 0, *self.y_rows(s, d))
            net.send(part, part, self.yz[s - 1][d], net.to_z(k))

    def yz_wait(self, s):
        for d, k in enumerate((1, -1)):
            self.net.arrived(self.slot(-k * s, 0, *self.y_rows(s, d)), self.yz[s - 1][d])

    def yb_send(self, lo, *kzs):
        net = self.net
        for kz in kzs:
            part = self.slot(kz, 0, lo, lo + 64)
            for d, k in enumerate((1, -1)):
                net.send(part, part, self.yb[lo][kz % NZ][d], net.to_y(k))

    def yf_send(self, lo, *kzs):
        net = self.net
        for kz in kzs:
            for d, k in enumerate((1, -1)):
                net.arrived(self.slot(kz, -k, lo, lo + 64), self.yb[lo][kz % NZ][d])
                part = self.slot(kz, -k, lo + 32 * d, lo + 32 * d + 32)
                net.send(part, part, self.yf[lo][kz % NZ][d], net.to_y(k))

    def yf_wait(self, lo, *kzs):
        for kz in kzs:
            for d in range(2):
                part = self.slot(kz, 2, lo + 32 * d, lo + 32 * d + 32)
                self.net.arrived(part, self.yf[lo][kz % NZ][d])


def rows_of(chunk, size=CH):
    return pl.ds(pl.multiple_of(chunk * size, size), size)


def iotas(n):
    return (
        lax.broadcasted_iota(jnp.int32, (n, n), 0),
        lax.broadcasted_iota(jnp.int32, (n, n), 1),
    )


class Attention:
    def __init__(self, net, r):
        self.net, self.r = net, r
        n = net.number
        self.m1 = [n() for _ in range(NY)]
        self.m2 = [n() for _ in range(NZ)]
        self.m3 = [n() for _ in range(NY)]
        self.heads = (
            (KA, r["ba"], r["sa"], r["ea"], r["pa"], r["ta"], 0),
            (KB, r["bb"], r["sb"], r["eb"], r["pb"], r["tb"], 1),
        )

    def load(self, kind, h, rows):
        if h == 0:
            return self.r[kind + "a"][rows, :].astype(F32)
        return self.r[kind + "b"][:, rows].astype(F32).T

    def states(self):
        r = self.r
        row, col = iotas(CH)
        lower = row >= col
        tri = jnp.where(lower, 1.0, 0.0).astype(BF16)
        tri2 = jnp.concatenate([tri, tri], axis=1)

        def step(c, carry):
            rows = rows_of(c)
            line = r["fade"][pl.ds(c, 1), :]
            fade = jnp.sum(jnp.where(lower, line, 0.0), axis=1, keepdims=True)
            new = []
            for (width, b, s, e, p, t, h), (state, before) in zip(self.heads, carry):
                x = self.load("g", h, rows)
                slow = (jnp.minimum(x, 0.0) - jnp.log1p(jnp.exp(-jnp.abs(x)))) * (1.0 / 16.0)
                high = slow.astype(BF16)
                low = (slow - high.astype(F32)).astype(BF16)
                sums = dot(tri2, jnp.concatenate([high, low], axis=0)) + fade
                b[rows, :] = sums
                total = sums[CH - 1 : CH, :]
                faded = (self.load("k", h, rows) * jnp.exp(total - sums)).astype(BF16)
                s[c] = state
                e[pl.ds(c, 1), :] = before
                state = jnp.exp(total) * state + dotg(r["v"][h, rows, :], faded, TD)
                new.append((state, before + total))
            return tuple(new)

        zero = tuple(
            (jnp.zeros((CH, width), F32), jnp.zeros((1, width), F32)) for width in (KA, KB)
        )
        (state_a, log_a), (state_b, log_b) = lax.fori_loop(0, NCH, step, zero, unroll=4)
        out = r["m1s"]
        quarter = CH // NY
        row16 = lax.broadcasted_iota(jnp.int32, (16, 1), 0)

        def two_rows(value):
            high = value.astype(BF16).astype(F32)
            return jnp.where(row16 == 0, high, value - high).astype(BF16)

        ends_a, ends_b = two_rows(jnp.exp(log_a)), two_rows(jnp.exp(log_b))
        for i in range(NY):
            part = slice(i * quarter, (i + 1) * quarter)
            out[i, 0:quarter, 0:KA] = state_a[part].astype(BF16)
            out[i, 0:quarter, KA : KA + KB] = state_b[part].astype(BF16)
            out[i, 0:quarter, KA + KB :] = jnp.zeros((quarter, KB), BF16)
            out[i, quarter:, 0:KA] = ends_a
            out[i, quarter:, KA : KA + KB] = ends_b
            out[i, quarter:, KA + KB :] = jnp.zeros((16, KB), BF16)

    def send_quarters(self):
        net, r = self.net, self.r
        for k in (2, 1, 3):
            net.send(r["m1s"].at[net.at_y(k)], r["m1r"].at[k], self.m1[k], net.to_y(k))

    @staticmethod
    def opened(message):
        quarter = CH // NY
        state = message[0:quarter, :].astype(F32)
        decay = message[quarter : quarter + 1, :].astype(F32) + message[
            quarter + 1 : quarter + 2, :
        ].astype(F32)
        return state, decay

    def send_line_total(self):
        net, r = self.net, self.r
        quarter = CH // NY
        for k in range(1, NY):
            net.arrived(r["m1r"].at[k], self.m1[k])
        r["m1r"][0] = r["m1s"][net.y]
        state = jnp.zeros((quarter, 256), F32)
        decay = jnp.ones((1, 256), F32)
        for i in range(NY):
            slot = lax.rem(net.y - i + NY, NY)
            own, factor = self.opened(r["m1r"][slot])
            state, decay = factor * state + own, factor * decay
        row16 = lax.broadcasted_iota(jnp.int32, (16, 1), 0)
        high = decay.astype(BF16).astype(F32)
        r["m2s"][0:quarter, :] = state.astype(BF16)
        r["m2s"][quarter:, :] = jnp.where(row16 == 0, high, decay - high).astype(BF16)
        for k in (4, 3, 5, 2, 6, 1, 7):

            @pl.when(net.z + k < NZ)
            def _():
                self.line_copy(k).start()

    def line_copy(self, k):
        net, r = self.net, self.r
        return net._copy(r["m2s"], r["m2r"].at[k], self.m2[k], net.to_z(k))

    def send_incoming(self):
        net, r = self.net, self.r
        quarter = CH // NY
        for k in range(1, NZ):

            @pl.when(k <= net.z)
            def _():
                net.arrived(r["m2r"].at[k], self.m2[k])

        state = jnp.zeros((quarter, 256), F32)
        for i in range(NZ - 1):
            slot = lax.rem(net.z - i + NZ, NZ)
            own, factor = self.opened(r["m2r"][slot])
            state = jnp.where(i < net.z, factor * state + own, state)
        for i in range(NY):
            r["m3s"][i] = state.astype(BF16)
            slot = lax.rem(net.y - i + NY, NY)
            own, factor = self.opened(r["m1r"][slot])
            state = factor * state + own
        for k in (2, 1, 3):
            net.send(r["m3s"].at[net.at_y(k)], r["m3r"].at[net.y], self.m3[k], net.to_y(k))
        r["m3r"][net.y] = r["m3s"][net.y]

    def incoming(self):
        net, r = self.net, self.r
        for k in range(1, NZ):

            @pl.when(net.z + k < NZ)
            def _():
                self.line_copy(k).wait_send()

        for k in range(1, NY):
            net.arrived(r["m3r"].at[net.at_y(-k)], self.m3[k])

    def scores(self, start, stop):
        r = self.r
        row, col = iotas(CH)
        near = ((row >> 5) == (col >> 5)) & (row >= col)
        middle = ((row >> 6) == (col >> 6)) & ((row >> 5) > (col >> 5))
        far = (row >> 6) > (col >> 6)

        def around(sums, size, at):
            width = sums.shape[1]
            parts = sums.reshape(CH // size, size, width)
            return (parts - parts[:, at : at + 1, :]).reshape(CH, width)

        def step(c, carry):
            rows = rows_of(c)
            for width, b, s, e, p, t, h in self.heads:
                sums = b[rows, :]
                query = self.load("q", h, rows) * (width**-0.5)
                key = self.load("k", h, rows)
                t[rows, :] = (query * jnp.exp(sums)).astype(BF16)
                at = around(sums, 32, 15)
                local = dotg(
                    (query * jnp.exp(at)).astype(BF16), (key * jnp.exp(-at)).astype(BF16), DT
                )
                total = jnp.where(near, local, 0.0)
                for size, at, mask in ((64, 31, middle), (128, 63, far)):
                    f = jnp.exp(-jnp.abs(around(sums, size, at)))
                    wide = dotg((query * f).astype(BF16), (key * f).astype(BF16), DT)
                    total = jnp.where(mask, wide, total)
                p[c] = total.astype(BF16)
            return carry

        lax.fori_loop(start, stop, step, 0, unroll=4)

    def gated(self, first, count):
        r = self.r

        def step(i, carry):
            c = first + i
            rows = rows_of(c)
            before_state = r["m3r"][...].astype(F32).reshape(CH, 256)
            for width, b, s, e, p, t, h in self.heads:
                state = s[c] + jnp.exp(e[pl.ds(c, 1), :]) * before_state[:, h * KA : h * KA + width]
                out = dot(p[c], r["v"][h, rows, :]) + dotg(t[rows, :], state.astype(BF16), DT)
                inverse = lax.rsqrt(jnp.mean(out * out, axis=-1, keepdims=True) + EPS)
                gate = r["og"][h, rows, :].astype(F32)
                normed = out * inverse * r["gain"][h : h + 1, :]
                value = gate * jax.nn.sigmoid(gate) * normed
                r["gat"][rows, h * CH : (h + 1) * CH] = value.astype(BF16)
            return carry

        lax.fori_loop(0, count, step, 0, unroll=2)


HALF = 1024
BLK = 256
LEFT, RIGHT = slice(0, 512), slice(512, 1024)


class Reduce:
    def __init__(self, net, part, comb, hop, joined, direct):
        self.net, self.part, self.comb = net, part, comb
        self.hop, self.joined, self.direct = hop, joined, direct
        n = net.number
        self.h = [[n(), n()] for _ in range(2)]
        self.j = [[n(), n()] for _ in range(2)]
        self.d = [[n(), n()] for _ in range(2)]

    def send_far(self, *pieces):
        net = self.net
        for piece in pieces:
            rows = pl.ds(piece * CH, CH)
            for side, (k, cols) in enumerate(((1, LEFT), (-1, RIGHT))):
                net.send(
                    self.part.at[0, rows, cols],
                    self.hop.at[side, rows],
                    self.h[side][piece],
                    net.to_x(k),
                )

    def send_near(self, *pieces):
        net = self.net
        for piece in pieces:
            rows = pl.ds(piece * CH, CH)
            for side, (k, block, cols) in enumerate(((1, 1, RIGHT), (-1, 2, LEFT))):
                net.send(
                    self.part.at[block, rows, cols],
                    self.direct.at[side, rows],
                    self.d[side][piece],
                    net.to_x(k),
                )

    def join(self, *pieces):
        net = self.net
        for piece in pieces:
            rows = slice(piece * CH, (piece + 1) * CH)
            for side, (k, block, cols) in enumerate(((1, 1, LEFT), (-1, 2, RIGHT))):
                net.arrived(self.hop.at[side, rows], self.h[side][piece])
                both = self.part[block, rows, cols].astype(F32) + self.hop[side, rows, :].astype(
                    F32
                )
                self.comb[side, rows, :] = both.astype(BF16)
                net.send(
                    self.comb.at[side, rows],
                    self.joined.at[side, rows],
                    self.j[side][piece],
                    net.to_x(k),
                )

    def arrived(self, piece):
        net = self.net
        rows = slice(piece * CH, (piece + 1) * CH)
        for side in range(2):
            net.arrived(self.direct.at[side, rows], self.d[side][piece])
            net.arrived(self.joined.at[side, rows], self.j[side][piece])

    def total(self, own, rows):
        left = (
            own[rows, LEFT]
            + self.joined[0, rows, :].astype(F32)
            + self.direct[1, rows, :].astype(F32)
        )
        right = (
            own[rows, RIGHT]
            + self.joined[1, rows, :].astype(F32)
            + self.direct[0, rows, :].astype(F32)
        )
        return left, right


class Feed:
    def __init__(self, net, r):
        self.net, self.r = net, r
        n = net.number
        self.n_res, self.n_wo, self.n_out = n(), n(), n()
        self.n_ss = [n(), n()]
        self.n_dp = [n() for _ in range(4)]
        self.n_gat = [n() for _ in range(NX)]
        self.n_hid = [[n(), n()] for _ in range(NX)]
        self.ring = [[n(), n()] for _ in range(2)]
        self.far = [[n(), n()] for _ in range(2)]
        self.over = [[n(), n()] for _ in range(NX)]
        self.first = Reduce(net, r["p1"], r["c1"], r["h1"], r["j1"], r["d1"])
        self.second = Reduce(net, r["p2"], r["c2"], r["h2"], r["j2"], r["d2"])

    def cols(self, core):
        return pl.ds(pl.multiple_of(core * HALF, HALF), HALF)

    def block(self, k):
        return rows_of(self.net.at_x(k), BLK)

    def swap_inputs(self):
        net, r = self.net, self.r
        other = 1 - net.c
        net.send(
            r["res"].at[:, self.cols(other)], r["base"].at[net.c], self.n_res, net.partner()
        )
        net.send(r["wo"].at[:, :, self.cols(other)], r["wop"], self.n_wo, net.partner())

    def send_gated(self, k):
        net, r = self.net, self.r
        rows = self.block(k)
        net.send(r["gat"].at[rows], r["gatp"].at[rows], self.n_gat[k % NX], net.partner())

    def swapped_inputs(self):
        net, r = self.net, self.r
        net.arrived(r["wop"], self.n_wo)
        net.arrived(r["base"].at[1 - net.c], self.n_res)
        r["base"][net.c] = r["res"][:, self.cols(net.c)]

    def project(self, k):
        net, r = self.net, self.r
        rows = self.block(k)
        net.arrived(r["gatp"].at[rows], self.n_gat[k % NX])
        mine, theirs = r["gat"][rows, :], r["gatp"][rows, :]
        for side in range(2):
            cols = slice(side * 512, (side + 1) * 512)
            at = pl.ds(pl.multiple_of(net.c * HALF + side * 512, 512), 512)
            part = dot(mine, r["wo"][:, :, at].reshape(2 * CH, 512)) + dot(
                theirs, r["wop"][:, :, cols].reshape(2 * CH, 512)
            )
            if k == 0:
                r["own1"][:, cols] = part
            else:
                r["p1"][{2: 0, 1: 1, -1: 2}[k], :, cols] = part.astype(BF16)

    def middle(self, piece):
        net, r = self.net, self.r
        self.first.arrived(piece)
        rows = slice(piece * CH, (piece + 1) * CH)
        left, right = self.first.total(r["own1"], rows)
        base = r["base"].at[piece]
        mid_l = (base[:, LEFT].astype(F32) + left).astype(BF16)
        mid_r = (base[:, RIGHT].astype(F32) + right).astype(BF16)
        r["mid"][rows, LEFT] = mid_l
        r["mid"][rows, RIGHT] = mid_r
        mid_l, mid_r = mid_l.astype(F32), mid_r.astype(F32)
        squares = jnp.sum(mid_l * mid_l + mid_r * mid_r, axis=-1, keepdims=True)
        r["ss"][piece] = jnp.broadcast_to(squares, (CH, 128))
        net.send(r["ss"].at[piece], r["ssp"].at[piece], self.n_ss[piece], net.partner())
        net.arrived(r["ssp"].at[piece], self.n_ss[piece])
        inverse = lax.rsqrt((squares + r["ssp"][piece][:, 0:1]) * (1.0 / 2048.0) + EPS)
        gain = r["fgain"][:, self.cols(net.c)]
        start = pl.multiple_of(net.x * BLK + piece * CH, CH)
        for side, mid in ((LEFT, mid_l), (RIGHT, mid_r)):
            normed = (mid * inverse * gain[:, side]).astype(BF16)
            r["all"][net.c, pl.ds(start, CH), side] = normed

    def piece(self, k, half, side=slice(0, HALF), other=False):
        start = pl.multiple_of(self.net.at_x(k) * BLK + half * CH, CH)
        core = 1 - self.net.c if other else self.net.c
        return self.r["all"].at[core, pl.ds(start, CH), side]

    def over_send(self, k, half):
        part = self.piece(k, half)
        self.net.send(part, part, self.over[k % NX][half], self.net.partner())

    def over_wait(self, *pieces):
        for k, half in pieces:
            self.net.arrived(self.piece(k, half, other=True), self.over[k % NX][half])

    def rows_out(self, half):
        net = self.net
        part = self.piece(0, half)
        for d, k in enumerate((1, -1)):
            net.send(part, part, self.ring[d][half], net.to_x(k))
        self.over_send(0, half)

    def rows_on(self, half):
        net = self.net
        for d, (k, side) in enumerate(((1, LEFT), (-1, RIGHT))):
            net.arrived(self.piece(-k, half), self.ring[d][half])
            part = self.piece(-k, half, side)
            net.send(part, part, self.far[d][half], net.to_x(k))
            self.over_send(-k, half)

    def rows_far(self, half):
        for d, side in enumerate((LEFT, RIGHT)):
            self.net.arrived(self.piece(2, half, side), self.far[d][half])
        self.over_send(2, half)

    def rows(self, k, half):
        start = pl.multiple_of(self.net.at_x(k) * BLK + half * CH, CH)
        return pl.ds(start, CH)

    def hidden(self, *pieces):
        net, r = self.net, self.r
        self.over_wait(*pieces)
        blocks = [self.rows(*piece) for piece in pieces]

        def step(n, carry):
            at = pl.ds(pl.multiple_of(n * 256, 256), 256)
            lines = jnp.concatenate(
                [
                    jnp.concatenate([r["all"][0, rows, :], r["all"][1, rows, :]], axis=1)
                    for rows in blocks
                ],
                axis=0,
            )
            gate, up = (
                dot(lines, r["wg"][:, :, low : low + 64, at].reshape(2 * HALF, 256))
                for low in (0, UP)
            )
            value = (gate * jax.nn.sigmoid(gate) * up).astype(BF16)
            for i, rows in enumerate(blocks):
                r["hid"][rows, at] = value[i * CH : (i + 1) * CH]
            return carry

        lax.fori_loop(0, FF // 256, step, 0)
        for (k, half), rows in zip(pieces, blocks):
            net.send(
                r["hid"].at[rows], r["hidp"].at[rows], self.n_hid[k % NX][half], net.partner()
            )

    def swap_tile(self, kz):
        net, r = self.net, self.r
        z = net.at_z(kz)

        @pl.when(z // 4 == 1 - net.c)
        def _():
            n = lax.rem(z, 4)
            self.tile(z, n).start()

    def tile(self, z, n):
        r = self.r
        return self.net._copy(
            r["wg"].at[z, :, DOWN:], r["dp"].at[n], self.n_dp[0] + n, self.net.partner()
        )

    def swapped_down(self):
        for n in range(4):
            copy = self.tile(4 * (1 - self.net.c) + n, n)
            copy.wait_send()
            copy.wait_recv()

    def down(self, *pieces):
        net, r = self.net, self.r
        blocks = [self.rows(*piece) for piece in pieces]
        for (k, half), rows in zip(pieces, blocks):
            net.arrived(r["hidp"].at[rows], self.n_hid[k % NX][half])

        def step(n, carry):
            at = pl.ds(pl.multiple_of(n * 256, 256), 256)
            lines = jnp.concatenate(
                [
                    jnp.concatenate([r["hid"][rows, :], r["hidp"][rows, :]], axis=1)
                    for rows in blocks
                ],
                axis=0,
            )
            w = jnp.concatenate(
                [
                    r["wg"][4 * net.c + n, :, DOWN:, :].reshape(256, FF),
                    r["dp"][n].reshape(256, FF),
                ],
                axis=1,
            )
            part = dotg(lines, w, DT)
            for i, (k, half) in enumerate(pieces):
                mine = part[i * CH : (i + 1) * CH]
                rows = slice(half * CH, (half + 1) * CH)
                if k == 0:
                    r["own2"][rows, at] = mine
                else:
                    r["p2"][{2: 0, 1: 1, -1: 2}[k], rows, at] = mine.astype(BF16)
            return carry

        lax.fori_loop(0, HALF // 256, step, 0)

    def finish(self):
        net, r = self.net, self.r
        for piece in range(2):
            self.second.arrived(piece)
            rows = slice(piece * CH, (piece + 1) * CH)
            left, right = self.second.total(r["own2"], rows)
            r["outs"][piece, :, LEFT] = (r["mid"][rows, LEFT].astype(F32) + left).astype(BF16)
            r["outs"][piece, :, RIGHT] = (r["mid"][rows, RIGHT].astype(F32) + right).astype(BF16)
        net.send(r["outs"].at[1 - net.c], r["outp"], self.n_out, net.partner())

        @pl.when(net.c == 0)
        def _():
            r["lo"][...] = r["outs"][0]

        @pl.when(net.c == 1)
        def _():
            r["hi"][...] = r["outs"][1]

        net.arrived(r["outp"], self.n_out)

        @pl.when(net.c == 0)
        def _():
            r["hi"][...] = r["outp"][...]

        @pl.when(net.c == 1)
        def _():
            r["lo"][...] = r["outp"][...]


INPUTS = dict(
    ga=((1024, KA), BF16),
    gb=((KB, 1024), BF16),
    fade=((NCH, CH), F32),
    ka=((1024, KA), BF16),
    kb=((KB, 1024), BF16),
    v=((2, 1024, CH), BF16),
    gate=None,
    down=None,
    up=None,
    qa=((1024, KA), BF16),
    qb=((KB, 1024), BF16),
    res=((CH, 2048), BF16),
    wo=((2, CH, 2048), BF16),
    og=((2, 1024, CH), BF16),
    gain=((2, CH), F32),
    fgain=((1, 2048), F32),
)
SCRATCH = dict(
    wg=((NZ, NY, WR, FF), BF16),
    ba=((1024, KA), F32),
    bb=((1024, KB), F32),
    sa=((NCH, CH, KA), F32),
    sb=((NCH, CH, KB), F32),
    ea=((NCH, KA), F32),
    eb=((NCH, KB), F32),
    pa=((NCH, CH, CH), BF16),
    pb=((NCH, CH, CH), BF16),
    ta=((1024, KA), BF16),
    tb=((1024, KB), BF16),
    m1s=((NY, 48, 256), BF16),
    m1r=((NY, 48, 256), BF16),
    m2s=((48, 256), BF16),
    m2r=((NZ, 48, 256), BF16),
    m3s=((NY, 32, 256), BF16),
    m3r=((NY, 32, 256), BF16),
    gat=((1024, 256), BF16),
    gatp=((1024, 256), BF16),
    wop=((2, CH, HALF), BF16),
    base=((2, CH, HALF), BF16),
    own1=((BLK, HALF), F32),
    p1=((3, BLK, HALF), BF16),
    c1=((2, BLK, 512), BF16),
    h1=((2, BLK, 512), BF16),
    j1=((2, BLK, 512), BF16),
    d1=((2, BLK, 512), BF16),
    mid=((BLK, HALF), BF16),
    ss=((2, CH, 128), F32),
    ssp=((2, CH, 128), F32),
    all=((2, 1024, HALF), BF16),
    hid=((1024, FF), BF16),
    hidp=((1024, FF), BF16),
    dp=((4, NY, 64, FF), BF16),
    own2=((BLK, HALF), F32),
    p2=((3, BLK, HALF), BF16),
    c2=((2, BLK, 512), BF16),
    h2=((2, BLK, 512), BF16),
    j2=((2, BLK, 512), BF16),
    d2=((2, BLK, 512), BF16),
    outs=((2, CH, HALF), BF16),
    outp=((CH, HALF), BF16),
)
COPIES = 192


class Inputs:
    def __init__(self, net, r, given, sems):
        self.copies = {}
        for i, name in enumerate(INPUTS):
            if INPUTS[name] is None:
                lo = {"gate": 0, "up": UP, "down": DOWN}[name]
                dst = r["wg"].at[net.z, net.y, lo : lo + 64]
            else:
                dst = r[name]
            self.copies[name] = pltpu.make_async_copy(given[name], dst, sems.at[i])

    def fetch(self, *names):
        for name in names:
            self.copies[name].start()

    def ready(self, *names):
        for name in names:
            self.copies[name].wait()


def kernel(*refs):
    count = len(INPUTS)
    given = dict(zip(INPUTS, refs))
    held = [name for name in INPUTS if INPUTS[name] is not None]
    r = dict(zip(["lo", "hi"] + list(SCRATCH) + held, refs[count:]))
    isem, ssem, rsem = refs[-3:]
    net = Net(ssem, rsem)
    weights = Weights(net, r["wg"])
    attention = Attention(net, r)
    feed = Feed(net, r)
    assert net.count <= COPIES, net.count
    inputs = Inputs(net, r, given, isem)
    net.greet()
    inputs.fetch("gate", "up", "down", "ga", "gb", "fade", "ka", "kb", "v")
    inputs.ready("ga", "gb", "fade", "ka", "kb", "v")
    inputs.fetch("qa", "qb", "res", "wo", "og", "gain", "fgain")
    inputs.ready("gate", "up", "down")
    net.greeted()
    weights.yz_send(1)
    weights.x_out()
    attention.states()
    inputs.ready("qa", "qb", "res", "wo", "og", "gain", "fgain")
    attention.send_quarters()
    weights.yb_send(UP, 0)
    feed.swap_inputs()
    attention.scores(0, 8)
    attention.send_line_total()
    weights.x_forward()
    weights.yb_send(DOWN, 0)
    weights.yz_wait(1)
    weights.yz_send(2)
    weights.yb_send(UP, 1, -1)
    weights.x_forwarded()
    weights.xz_send(1)
    feed.swapped_inputs()
    weights.yf_send(UP, 0)
    attention.send_incoming()
    weights.yz_wait(2)
    weights.yz_send(3)
    weights.yb_send(DOWN, 1, -1)
    weights.yb_send(UP, 2, -2)
    attention.incoming()
    for k in (2, 1, -1, 0):
        attention.gated(2 * net.at_x(k), 2)
        feed.send_gated(k)
        if k == 1:
            feed.project(2)
            feed.first.send_far(0, 1)
    feed.project(1)
    feed.project(-1)
    feed.first.send_near(0, 1)
    feed.project(0)
    weights.yf_send(UP, 1, -1)
    weights.xz_wait(1)
    weights.xz_send(2)
    weights.yf_send(DOWN, 0)
    weights.yz_wait(3)
    weights.yz_send(4)
    weights.yb_send(UP, 3, -3)
    weights.yb_send(DOWN, 2, -2)
    weights.yf_send(UP, 2, -2)
    feed.first.join(0, 1)
    weights.yb_send(DOWN, 3, -3)
    weights.yf_send(DOWN, 1, -1)
    weights.xz_wait(2)
    weights.xz_send(3)
    feed.middle(0)
    feed.rows_out(0)
    weights.yz_wait(4)
    weights.yb_send(UP, 4)
    weights.yb_send(DOWN, 4)
    feed.middle(1)
    feed.rows_out(1)
    weights.yf_send(UP, 3, -3)
    weights.yf_send(DOWN, 2, -2)
    feed.rows_on(0)
    weights.xz_wait(3)
    weights.xz_send(4)
    weights.yf_send(UP, 4)
    weights.yf_send(DOWN, 3, -3, 4)
    feed.rows_on(1)
    for k in (0, 1, -1):
        weights.yf_wait(DOWN, k)
        feed.swap_tile(k)
    weights.yf_wait(UP, 0, 1, -1, 2, -2, 3, -3, 4)
    weights.xz_wait(4)
    feed.hidden((1, 0), (-1, 0))
    for k in (2, -2):
        weights.yf_wait(DOWN, k)
        feed.swap_tile(k)
    feed.hidden((1, 1), (-1, 1))
    feed.rows_far(0)
    feed.hidden((0, 0), (0, 1))
    for k in (3, -3, 4):
        weights.yf_wait(DOWN, k)
        feed.swap_tile(k)
    feed.rows_far(1)
    feed.hidden((2, 0), (2, 1))
    feed.swapped_down()
    feed.down((1, 0), (-1, 0))
    feed.second.send_near(0)
    feed.down((1, 1), (-1, 1))
    feed.second.send_near(1)
    feed.down((2, 0), (2, 1))
    feed.second.send_far(0, 1)
    feed.down((0, 0), (0, 1))
    feed.second.join(0, 1)
    feed.finish()
    net.drain()


def per_device(
    residual,
    first_group_queries,
    first_group_keys,
    second_group_queries,
    second_group_keys,
    primary_retain_switch_inputs,
    secondary_retain_switch_inputs,
    timestep_fading_exponent,
    values,
    output_gate_logits,
    head_norm_gains,
    output_projection,
    feedforward_norm_gain,
    gate_projection,
    up_projection,
    down_projection,
):
    given = dict(
        ga=primary_retain_switch_inputs,
        gb=secondary_retain_switch_inputs.T,
        fade=timestep_fading_exponent.reshape(NCH, CH),
        ka=first_group_keys,
        kb=second_group_keys.T,
        v=values,
        gate=gate_projection,
        down=down_projection.T,
        up=up_projection,
        qa=first_group_queries,
        qb=second_group_queries.T,
        res=residual,
        wo=output_projection,
        og=output_gate_logits,
        gain=head_norm_gains,
        fgain=feedforward_norm_gain.reshape(1, -1),
    )
    half = jax.ShapeDtypeStruct((CH, HALF), BF16)
    buffers = list(SCRATCH.values()) + [spec for spec in INPUTS.values() if spec is not None]
    lo, hi = pl.pallas_call(
        kernel,
        out_shape=(half, half),
        in_specs=[pl.BlockSpec(memory_space=pl.ANY)] * len(INPUTS),
        out_specs=(pl.BlockSpec(memory_space=pltpu.VMEM),) * 2,
        scratch_shapes=[pltpu.VMEM(shape, dtype) for shape, dtype in buffers]
        + [
            pltpu.SemaphoreType.DMA((len(INPUTS),)),
            pltpu.SemaphoreType.DMA((COPIES,)),
            pltpu.SemaphoreType.DMA((COPIES,)),
        ],
        compiler_params=pltpu.CompilerParams(
            collective_id=0, has_side_effects=True, vmem_limit_bytes=66000000
        ),
    )(*(given[name] for name in INPUTS))
    return jnp.concatenate([lo, hi], axis=1)


def solution(mesh):
    finer = Mesh(mesh.devices.reshape(NZ, NY, NX, 2), SP_TP)
    return jax.shard_map(
        per_device,
        mesh=finer,
        in_specs=(
            P(SP_TP, None),
            P(SP, TP),
            P(SP, TP),
            P(SP, TP),
            P(SP, TP),
            P(SP, TP),
            P(SP, TP),
            P(SP),
            P(None, SP, TP),
            P(None, SP, TP),
            P(None, TP),
            P(None, TP, None),
            P(),
            P(SP, TP),
            P(SP, TP),
            P(TP, SP),
        ),
        out_specs=P(SP_TP, None),
        check_vma=False,
    )
```
